512 devices in a mesh: kv: 64 (over z, y), tp: 8 (over x, core).
Axes of the slice: x: 4, y: 8, z: 8, core: 2. Of those that a mesh axis runs over, the one named last changes fastest.
Arguments:
- queries: bfloat16 [8192, 1024], P('kv', 'tp'), may hold values from -4 to 4
- keys: bfloat16 [8192, 1024], P('kv', 'tp'), may hold values from -4 to 4
- values: bfloat16 [8192, 1024], P('kv', 'tp'), may hold values from -4 to 4
- cotangent: bfloat16 [8192, 1024], P('kv', 'tp'), may hold values from -4 to 4
- log_sum: float32 [16, 8192], P('tp', 'kv'), may hold values from 4.5 to 7.5
- chosen: int32 [16, 256, 12], P('tp'), may hold values from 0 to 255, as said below
- normed_input: bfloat16 [8192, 2048], P('kv', 'tp'), may hold values from -0.0625 to 0.0625
Outputs:
- grad_queries: bfloat16 [8192, 1024], P('kv', 'tp')
- grad_keys: bfloat16 [8192, 1024], P('kv', 'tp')
- grad_values: bfloat16 [8192, 1024], P('kv', 'tp')
- grad_weight: float32 [2048, 1024], P('kv', 'tp')
The draws below stay inside these ranges and needn't reach their ends.
Inputs may be any that keep to these rules, and one draw needn't show every extreme that they name: `chosen`: for each head, the distinct blocks below their own query block that the query blocks of one device's 128 positions choose include at most 1 block of any one device's span of 128 positions, and exactly 1 for some pairs of devices. Within one list the entries below the query block's own index are distinct.
All inputs are finite; a program needn't handle non-finite values.
Results may differ from the reference program's by a relative error of at most 0.0085.
Values may be sent and summed in bfloat16 or wider, within the bound.
A program may use at most 64 MiB of HBM per device.

```python
import jax
import jax.numpy as jnp
from jax import lax

D = 2048
HEADS = 16
HD = 64
BLK = 32
SEL = 12
MOST = 1
TOK_DEV = 128
TOKENS = 8192
WIDTH = 1024
N_KV = 64


def draw_chosen(key, part):
    devices = N_KV
    blocks_dev = TOK_DEV // BLK
    splits = jax.random.split(jax.random.fold_in(key, 17), 4)
    first_pick = jax.random.randint(splits[0], (HEADS, devices, devices), 0, blocks_dev)
    step_pick = jax.random.randint(splits[1], (HEADS, devices, devices), 1, blocks_dev)
    owner_ids = jnp.arange(devices, dtype=jnp.int32)
    cand_list = []
    for slot_index in range(MOST):
        local_pick = (first_pick + slot_index * step_pick) % blocks_dev
        cand_list.append(owner_ids[None, None, :] * blocks_dev + local_pick)
    candidates = jnp.stack(cand_list, axis=-1)
    popular = jax.random.randint(splits[2], (HEADS, 1, devices, 1), 0, 8)
    popular = popular * popular
    query_dev = owner_ids[None, :, None, None]
    owner_dev = owner_ids[None, None, :, None]
    boosted = jnp.where((owner_dev == query_dev - 1) | (owner_dev == query_dev - devices // 2), 2, 0)
    base_score = boosted * 64 + popular
    jitter = jax.random.randint(splits[3], (HEADS, devices, blocks_dev, devices, MOST), 0, 4096)
    query_ids = owner_ids[:, None] * blocks_dev + jnp.arange(blocks_dev, dtype=jnp.int32)[None, :]
    cand_rows = candidates[:, :, None, :, :]
    usable = cand_rows < query_ids[None, :, :, None, None]
    tie_break = jnp.arange(MOST * devices, dtype=jnp.int32).reshape(devices, MOST)
    scored = (base_score[:, :, None, :, :] * 4096 + jitter) * 256 + tie_break
    scored = jnp.where(usable, scored, -1).reshape(HEADS, devices, blocks_dev, MOST * devices)
    top_values, top_index = lax.top_k(scored, SEL)
    flat_cands = jnp.broadcast_to(cand_rows, (HEADS, devices, blocks_dev, devices, MOST)).reshape(HEADS, devices, blocks_dev, MOST * devices)
    picked = jnp.take_along_axis(flat_cands, top_index, axis=-1)
    picked = jnp.where(top_values >= 0, picked, query_ids[None, :, :, None])
    return picked.reshape(HEADS, devices * blocks_dev, SEL).astype(jnp.int32)


def block_levels(stream_key, shape, cuts, low, largest):
    level, own = 1.0, jax.random.fold_in(stream_key, 6)
    for dim, blocks in cuts:
        draws = jnp.exp(jax.random.uniform(jax.random.fold_in(own, dim), (blocks,), jnp.float32, low / len(cuts), largest / len(cuts)))
        level = level * jnp.repeat(draws, shape[dim] // blocks).reshape([-1 if axis == dim else 1 for axis in range(len(shape))])
    return level


def noise(own_key, shape, scale, most, pieces=(), kind=jnp.bfloat16):
    gain = block_levels(own_key, shape, pieces, -0.22, 0.18) if pieces else 1.0
    array = jax.random.normal(own_key, shape, jnp.float32) * scale * gain
    return jnp.minimum(jnp.maximum(array, -most), most).astype(kind)


def setup_inputs(seed: int = 0) -> dict:
    key_list = jax.random.split(jax.random.key(seed), 8)
    queries = noise(key_list[0], (TOKENS, WIDTH), 1.0, 4.0, ((0, 64), (1, 8)))
    keys = noise(key_list[1], (TOKENS, WIDTH), 1.0, 4.0, ((0, 64), (1, 8)))
    values = noise(key_list[2], (TOKENS, WIDTH), 1.0, 4.0, ((0, 64), (1, 8)))
    cotangent = noise(key_list[3], (TOKENS, WIDTH), 1.0, 4.0, ((0, 64), (1, 8)))
    log_sum = jnp.clip(4.5 + 3.0 * jax.random.uniform(key_list[4], (HEADS, TOKENS), jnp.float32) ** block_levels(key_list[4], (HEADS, TOKENS), ((0, 8), (1, 64)), -0.2, 0.2), 4.5, 7.5)
    chosen = draw_chosen(jax.random.fold_in(key_list[7], 71), 0)
    normed_input = noise(key_list[6], (TOKENS, D), TOKENS ** -0.5, 0.0625, ((0, 64), (1, 8)))
    return dict(queries=queries, keys=keys, values=values, cotangent=cotangent, log_sum=log_sum, chosen=chosen, normed_input=normed_input)


MASKED = -1e30


def reference(queries, keys, values, cotangent, log_sum, chosen, normed_input):
    token_count = queries.shape[0]
    block_total = token_count // BLK
    score_scale = HD ** -0.5
    block_ids = jnp.arange(block_total, dtype=jnp.int32)
    causal = jnp.arange(BLK)[:, None] >= jnp.arange(BLK)[None, :]

    def per_head(head_index):
        def columns(row_block):
            picked_cols = lax.dynamic_slice_in_dim(row_block, head_index * HD, HD, 1)
            return picked_cols.reshape(block_total, BLK, HD).astype(jnp.float32)

        q_blocks = columns(queries)
        k_blocks = columns(keys)
        v_blocks = columns(values)
        g_blocks = columns(cotangent)
        log_rows = lax.dynamic_index_in_dim(log_sum, head_index, 0, keepdims=False).reshape(block_total, BLK)[..., None]
        picked = lax.dynamic_index_in_dim(chosen, head_index, 0, keepdims=False).astype(jnp.int32)
        usable = picked < block_ids[:, None]
        safe_ids = jnp.where(usable, picked, 0).astype(jnp.int32)
        keys_all = jnp.concatenate([k_blocks[safe_ids].reshape(block_total, SEL * BLK, HD), k_blocks], axis=1)
        values_all = jnp.concatenate([v_blocks[safe_ids].reshape(block_total, SEL * BLK, HD), v_blocks], axis=1)
        sel_mask = jnp.broadcast_to(jnp.repeat(usable, BLK, axis=1)[:, None, :], (block_total, BLK, SEL * BLK))
        allowed = jnp.concatenate([sel_mask, jnp.broadcast_to(causal, (block_total, BLK, BLK))], axis=2)
        scores = jnp.einsum('jqd,jkd->jqk', q_blocks, keys_all) * score_scale
        weights = jnp.exp(jnp.where(allowed, scores - log_rows, MASKED))
        value_dots = jnp.einsum('jqd,jkd->jqk', g_blocks, values_all)
        row_delta = jnp.sum(weights * value_dots, axis=-1, keepdims=True)
        score_grad = lax.optimization_barrier((weights * (value_dots - row_delta)).astype(jnp.bfloat16)).astype(jnp.float32)
        weights_low = lax.optimization_barrier(weights.astype(jnp.bfloat16)).astype(jnp.float32)
        query_grad = jnp.einsum('jqk,jkd->jqd', score_grad, keys_all) * score_scale
        key_grad = jnp.einsum('jqk,jqd->jkd', score_grad, q_blocks) * score_scale
        value_grad = jnp.einsum('jqk,jqd->jkd', weights_low, g_blocks)

        def settle(gradient):
            spread = gradient[:, :SEL * BLK].reshape(block_total * SEL, BLK, HD)
            summed = jax.ops.segment_sum(spread, safe_ids.reshape(-1), num_segments=block_total)
            return (summed + gradient[:, SEL * BLK:]).reshape(token_count, HD).astype(jnp.bfloat16)

        return query_grad.reshape(token_count, HD).astype(jnp.bfloat16), settle(key_grad), settle(value_grad)

    head_grads = lax.map(per_head, jnp.arange(HEADS, dtype=jnp.int32))

    def joined_rows(stacked):
        return stacked.transpose(1, 0, 2).reshape(token_count, HEADS * HD)

    grad_queries = joined_rows(head_grads[0])
    grad_keys = joined_rows(head_grads[1])
    grad_values = joined_rows(head_grads[2])
    grad_weight = jnp.dot(normed_input.T, grad_queries, preferred_element_type=jnp.float32)
    return grad_queries, grad_keys, grad_values, grad_weight
```

```python
import functools

import jax
import jax.numpy as jnp
from jax import lax
from jax.experimental import pallas as pl
from jax.experimental.pallas import tpu as pltpu
from jax.sharding import PartitionSpec as P

HD = 64
BLK = 32
MASKED = -1e30
MESH = pl.DeviceIdType.MESH
F32 = jnp.float32
BF16 = jnp.bfloat16


def dot(a, b, ca, cb):
    return lax.dot_general(a, b, (((ca,), (cb,)), ((), ())), preferred_element_type=F32)


def iota(shape, dim):
    return lax.broadcasted_iota(jnp.int32, shape, dim)


def each(low, high, fn):
    def step(i, carry):
        fn(i)
        return carry
    lax.fori_loop(low, high, step, 0)


def kernel(
    g, r, tp, q_in, k_in, v_in, c_in, lse_in, pick_in, x_in,
    gq_ref, gk_ref, gv_ref, gw_ref,
    q_ref, k_ref, v_ref, c_ref, lse_ref, pick_ref, x_ref, insem,
    qs, cs, hot, bias, kz, kvs, kvt, wts, vds, back_s, back_r, rel_s, rel_r, gko, gvo, dqa,
    xs, xg, xr, dqr, gs, gr,
    zs_sem, zr_sem, ys_sem, yr_sem, bs_sem, br_sem, rs_sem, rr_sem,
    x1s, x1r, x2s, x2r, dqs_sem, dqr_sem, gs_sem, gr_sem,
):
    tok, cols = q_ref.shape
    sel, heads, blocks = pick_ref.shape
    bd = tok // BLK
    wide = 2 * tok
    chunk = g * BLK
    scale = HD ** (-0.5)
    me, t = lax.axis_index("kv"), lax.axis_index("tp")
    z, y = me // g, lax.rem(me, g)

    loads = {}
    for i, (a, b) in enumerate((
        (pick_in, pick_ref), (k_in, k_ref), (v_in, v_ref), (x_in, x_ref),
        (q_in, q_ref), (c_in, c_ref), (lse_in, lse_ref),
    )):
        loads[i] = pltpu.make_async_copy(a, b, insem.at[i])
        loads[i].start()

    barrier = pltpu.get_barrier_semaphore()

    def greet(kv, tt):
        pl.semaphore_signal(barrier, inc=1, device_id=(kv, tt), device_id_type=MESH)

    for i in range(1, r):
        greet(lax.rem(z + i, r) * g + y, t)
    for i in range(1, g):
        greet(z * g + lax.rem(y + i, g), t)
    for i in range(1, tp):
        greet(me, lax.rem(t + i, tp))
    for i in range(r):
        zz = lax.rem(z + i, r)
        if i == 0:
            @pl.when(t != z)
            def _():
                greet(zz * g + y, z)
        else:
            greet(zz * g + y, z)

    def z_copy(c, zz, slot):
        return pltpu.make_async_remote_copy(
            src_ref=(k_ref, v_ref)[c], dst_ref=kz.at[slot, c], send_sem=zs_sem.at[c, zz],
            recv_sem=zr_sem.at[c, slot], device_id=(zz * g + y, t), device_id_type=MESH)

    def y_copy(zz, yy, slot):
        return pltpu.make_async_remote_copy(
            src_ref=kvs.at[zz, yy], dst_ref=kvt.at[zz * g + slot], send_sem=ys_sem.at[zz, yy],
            recv_sem=yr_sem.at[zz, slot], device_id=(z * g + yy, t), device_id_type=MESH)

    def back_copy(c, zz, yy, slot):
        return pltpu.make_async_remote_copy(
            src_ref=back_s.at[c, zz, yy], dst_ref=back_r.at[c, zz, slot], send_sem=bs_sem.at[c, zz, yy],
            recv_sem=br_sem.at[c, zz, slot], device_id=(z * g + yy, t), device_id_type=MESH)

    def rel_copy(c, zz, slot):
        return pltpu.make_async_remote_copy(
            src_ref=rel_s.at[c, zz], dst_ref=rel_r.at[c, slot], send_sem=rs_sem.at[c, zz],
            recv_sem=rr_sem.at[c, slot], device_id=(zz * g + y, t), device_id_type=MESH)

    def x1_copy(s, slot):
        return pltpu.make_async_remote_copy(
            src_ref=xs.at[s], dst_ref=xg.at[slot], send_sem=x1s.at[s], recv_sem=x1r.at[slot],
            device_id=(t * g + y, s), device_id_type=MESH)

    def x2_copy(tt, slot):
        return pltpu.make_async_remote_copy(
            src_ref=xg, dst_ref=xr.at[slot], send_sem=x2s.at[tt], recv_sem=x2r.at[slot],
            device_id=(me, tt), device_id_type=MESH)

    def dq_copy(zz, slot):
        return pltpu.make_async_remote_copy(
            src_ref=dqr.at[z], dst_ref=dqr.at[slot], send_sem=dqs_sem.at[zz], recv_sem=dqr_sem.at[slot],
            device_id=(zz * g + y, t), device_id_type=MESH)

    def gw_copy(yy, slot):
        return pltpu.make_async_remote_copy(
            src_ref=gs.at[yy], dst_ref=gr.at[slot], send_sem=gs_sem.at[yy], recv_sem=gr_sem.at[slot],
            device_id=(z * g + yy, t), device_id_type=MESH)

    def each_x1(low, fn):
        def step(s):
            @pl.when((t != z) | (s != t))
            def _():
                fn(s)
        each(low, tp, step)

    def each_x1_in(fn):
        def step(zz):
            @pl.when((t != z) | (zz != z))
            def _():
                fn(zz)
        each(0, r, step)

    loads[0].wait()
    row_of = iota((blocks, heads * g * bd), 0) - z * (g * bd)
    col_of = iota((blocks, heads * g * bd), 1)
    at_row = lax.rem(col_of, g * bd) == row_of
    at_tok = me * bd + lax.rem(iota((blocks, heads * tok), 1), tok) // BLK == iota((blocks, heads * tok), 0)
    tok_head = iota((blocks, heads * tok), 1) // tok
    row_ids, ids = None, None
    for h in range(heads):
        mine = pick_ref[:, h, :].astype(F32).astype(BF16)
        pick_row = (at_row & (col_of // (g * bd) == h)).astype(F32).astype(BF16)
        pick_tok = (at_tok & (tok_head == h)).astype(F32).astype(BF16)
        a, b = dot(mine, pick_row, 1, 0), dot(mine, pick_tok, 1, 0)
        row_ids = a if row_ids is None else row_ids + a
        ids = b if ids is None else ids + b
    row_ids = (row_ids + 0.5).astype(jnp.int32)
    ids = (ids + 0.5).astype(jnp.int32)
    ids = jnp.where(ids < me * bd + lax.rem(iota(ids.shape, 1), tok) // BLK, ids, blocks)
    target_at = iota((r * bd, heads * g * bd), 0)
    target = (target_at // bd * g + y) * bd + lax.rem(target_at, bd)
    hit = jnp.zeros(target.shape, F32)
    for s in range(sel):
        hit = jnp.where(row_ids[s : s + 1, :] == target, 1.0, hit)
    out_at, out_from = iota((heads * g * bd, g * cols), 1), iota((heads * g * bd, g * cols), 0)
    fan = (lax.rem(out_from, g * bd) // bd == out_at // cols) & (
        lax.rem(out_at, cols) // HD == out_from // (g * bd))
    taken = dot(hit.astype(BF16), fan.astype(F32).astype(BF16), 1, 0)
    taken = jnp.where(taken > 0.5, 1.0, 0.0).reshape(r, bd, g * cols)
    for yy in range(g):
        hot[:, yy] = taken[:, :, yy * cols : (yy + 1) * cols]

    loads[1].wait()
    loads[2].wait()
    pl.semaphore_wait(barrier, (r - 1) + (g - 1) + (tp - 1) + r - jnp.where(t == z, 1, 0))

    def span(i):
        zz = r - 1 - i
        z_copy(0, zz, z).start()
        z_copy(1, zz, z).start()
    each(0, r - 1 - z, span)

    def mask(zz, yy, b):
        return jnp.broadcast_to(hot[zz, yy, pl.ds(b, 1), :], (BLK, cols))

    def picked(zz, yy, k_from, v_from):
        k_out, v_out = None, None
        for b in range(bd):
            one = mask(zz, yy, b).astype(BF16)
            k_term, v_term = k_from(b) * one, v_from(b) * one
            k_out = k_term if k_out is None else k_out + k_term
            v_out = v_term if v_out is None else v_out + v_term
        return k_out, v_out

    def own_rows(i):
        yy = y + 1 + i
        a, b = picked(z, yy, lambda b: k_ref[b * BLK : (b + 1) * BLK, :], lambda b: v_ref[b * BLK : (b + 1) * BLK, :])
        kvs[z, yy, 0] = a
        kvs[z, yy, 1] = b
        y_copy(z, yy, y).start()
    each(0, g - 1 - y, own_rows)

    loads[3].wait()
    width = x_ref.shape[1]
    w = width // tp
    eye = (iota((width, width), 0) == iota((width, width), 1)).astype(F32).astype(BF16)
    flipped = dot(eye, x_ref[...], 1, 1).astype(BF16)
    xs[...] = flipped.reshape(tp, w, tok)
    each_x1(0, lambda s: x1_copy(s, z).start())

    @pl.when(t == z)
    def _():
        xg[z] = xs[t]

    def clear(yy):
        kvt[z * g + yy] = jnp.zeros(kvt.shape[1:], BF16)
    each(y, g, clear)

    for i in (4, 5, 6):
        loads[i].wait()
    less = jnp.concatenate([-lse_ref[h : h + 1, :] for h in range(heads)], axis=1)
    owner = ids // bd
    for zz in range(r):
        need = jnp.zeros((g, wide), jnp.bool_)
        at = zz * g + iota((g, wide), 0)
        for s in range(sel):
            need = need | (owner[s : s + 1, :] == at)
        bias[zz] = jnp.where(need & (at < me), less, MASKED)
    low = iota((tok, cols), 1) < HD

    def stacked(ref):
        part = ref[...]
        zero = jnp.zeros_like(part)
        return jnp.concatenate([jnp.where(low, part, zero), jnp.where(low, zero, part)], axis=0)

    qs[...] = stacked(q_ref)
    cs[...] = stacked(c_ref)

    def relay(i):
        zz = z - 1 - i
        z_copy(0, zz, zz).wait_recv()
        z_copy(1, zz, zz).wait_recv()

        def one(k):
            yy = lax.rem(y + k, g)
            a, b = picked(zz, yy, lambda b: kz[zz, 0, b * BLK : (b + 1) * BLK, :],
                          lambda b: kz[zz, 1, b * BLK : (b + 1) * BLK, :])

            @pl.when(k != g)
            def _():
                kvs[zz, yy, 0] = a
                kvs[zz, yy, 1] = b
                y_copy(zz, yy, y).start()

            @pl.when(k == g)
            def _():
                kvt[zz * g + y, 0] = a
                kvt[zz * g + y, 1] = b
        each(1, g + 1, one)
    each(0, z, relay)

    each_x1_in(lambda zz: x1_copy(0, zz).wait_recv())
    for i in range(1, tp):
        x2_copy(lax.rem(t + i, tp), t).start()
    xr[t] = xg[...]

    key_at = iota((tok, wide), 0)
    query_at = lax.rem(iota((tok, wide), 1), tok)
    own_block = key_at // BLK
    need = jnp.zeros((tok, wide), jnp.bool_)
    own_ids = jnp.where(owner == me, lax.rem(ids, bd), bd)
    for s in range(sel):
        need = need | (own_ids[s : s + 1, :] == own_block)
    need = need | ((own_block == query_at // BLK) & (key_at <= query_at))
    own = jnp.exp(dot(k_ref[...], qs[...], 1, 1) * scale + jnp.where(need, less, MASKED))
    vdo = dot(v_ref[...], cs[...], 1, 1)
    gvo[...] = dot(own.astype(BF16), cs[...], 1, 0)
    first = jnp.sum(own * vdo, axis=0, keepdims=True)

    def send_back(c, zz):
        def one(k):
            yy = lax.rem(y + k, g)

            @pl.when((zz < z) | (yy < y))
            def _():
                back_copy(c, zz, yy, y).start()
        each(1, g, one)

    def pass_one(i, delta):
        zz = z - i

        def arrive(k):
            yy = lax.rem(y + k, g)

            @pl.when((zz < z) | (yy < y))
            def _():
                y_copy(zz, 0, yy).wait_recv()
        each(1, g, arrive)
        kp = kvt[pl.ds(zz * g, g), 0].reshape(chunk, cols)
        vp = kvt[pl.ds(zz * g, g), 1].reshape(chunk, cols)
        line = jnp.concatenate(
            [jnp.broadcast_to(bias[zz, a : a + 1, :], (BLK, wide)) for a in range(g)], axis=0)
        weights = jnp.exp(dot(kp, qs[...], 1, 1) * scale + line)
        vd = dot(vp, cs[...], 1, 1)
        wts[zz] = weights
        vds[zz] = vd
        back_s[1, zz] = dot(weights.astype(BF16), cs[...], 1, 0).astype(BF16).reshape(g, BLK, cols)
        send_back(1, zz)
        return delta + jnp.sum(weights * vd, axis=0, keepdims=True)
    delta = lax.fori_loop(0, z + 1, pass_one, first)

    dso = (own * (vdo - delta)).astype(BF16)
    dqa[...] = dot(dso, k_ref[...], 0, 0)

    def pass_two(i):
        zz = z - i
        kp = kvt[pl.ds(zz * g, g), 0].reshape(chunk, cols)
        ds = (wts[zz] * (vds[zz] - delta)).astype(BF16)
        dqa[...] += dot(ds, kp, 0, 0)
        back_s[0, zz] = (dot(ds, qs[...], 1, 0) * scale).astype(BF16).reshape(g, BLK, cols)
        send_back(0, zz)
    each(0, z + 1, pass_two)

    dq = jnp.where(low, dqa[:tok], dqa[tok:]) * scale
    dq = dq.astype(BF16)
    gq_ref[...] = dq
    dqr[z] = dq
    for i in range(1, r):
        dq_copy(lax.rem(z + i, r), z).start()
    gko[...] = dot(dso, qs[...], 1, 0) * scale

    def relay_back(c):
        own_sum = gko if c == 0 else gvo

        def own_add(i):
            yy = y + 1 + i
            back_copy(c, z, 0, yy).wait_recv()
            got = back_r[c, z, yy].astype(F32)
            for b in range(bd):
                own_sum[b * BLK : (b + 1) * BLK, :] += got * mask(z, yy, b)

        def one(i):
            zz = z - 1 - i
            sums = [back_s[c, zz, y].astype(F32) * mask(zz, y, b) for b in range(bd)]

            def add(k, acc):
                yy = lax.rem(y + k, g)
                back_copy(c, zz, 0, yy).wait_recv()
                got = back_r[c, zz, yy].astype(F32)
                return tuple(acc[b] + got * mask(zz, yy, b) for b in range(bd))
            sums = lax.fori_loop(1, g, add, tuple(sums))
            for b in range(bd):
                rel_s[c, zz, b * BLK : (b + 1) * BLK, :] = sums[b].astype(BF16)
            rel_copy(c, zz, z).start()
        each(0, z, one)
        each(0, g - 1 - y, own_add)

    relay_back(1)

    for i in range(1, tp):
        tt = lax.rem(t + i, tp)
        x2_copy(tt, tt).wait_recv()
    total = None
    for zz in range(r):
        @pl.when(zz != z)
        def _():
            dq_copy(zz, zz).wait_recv()
        part = dot(xr[:, zz].reshape(width, tok), dqr[zz], 1, 0)
        total = part if total is None else total + part
    for yy in range(g):
        gs[yy] = total[yy * w : (yy + 1) * w].astype(BF16)

        @pl.when(yy == y)
        def _():
            gw_ref[...] = total[yy * w : (yy + 1) * w]
    for i in range(1, g):
        gw_copy(lax.rem(y + i, g), y).start()

    relay_back(0)

    for i in range(1, g):
        yy = lax.rem(y + i, g)
        gw_copy(yy, yy).wait_recv()
        gw_ref[...] += gr[yy].astype(F32)

    def settle(c):
        own_sum = gko if c == 0 else gvo

        def one(i):
            zz = z + 1 + i
            rel_copy(c, 0, zz).wait_recv()
            own_sum[...] += rel_r[c, zz].astype(F32)
        each(0, r - 1 - z, one)
        (gk_ref if c == 0 else gv_ref)[...] = own_sum[...].astype(BF16)
    settle(1)
    settle(0)

    def sent_span(i):
        z_copy(0, z + 1 + i, z).wait_send()
        z_copy(1, z + 1 + i, z).wait_send()
    each(0, r - 1 - z, sent_span)
    each(0, g - 1 - y, lambda i: y_copy(z, y + 1 + i, y).wait_send())

    def sent_row(zz):
        def one(k):
            yy = lax.rem(y + k, g)
            y_copy(zz, yy, y).wait_send()
        each(1, g, one)
        rel_copy(0, zz, z).wait_send()
        rel_copy(1, zz, z).wait_send()
    each(0, z, sent_row)

    def sent_back(zz):
        def one(k):
            yy = lax.rem(y + k, g)

            @pl.when((zz < z) | (yy < y))
            def _():
                back_copy(0, zz, yy, y).wait_send()
                back_copy(1, zz, yy, y).wait_send()
        each(1, g, one)
    each(0, z + 1, sent_back)
    each_x1(0, lambda s: x1_copy(s, z).wait_send())
    for i in range(1, tp):
        x2_copy(lax.rem(t + i, tp), t).wait_send()
    for i in range(1, r):
        dq_copy(lax.rem(z + i, r), z).wait_send()
    for i in range(1, g):
        gw_copy(lax.rem(y + i, g), y).wait_send()


def write_out(*refs):
    sems = refs[8]
    copies = [pltpu.make_async_copy(refs[i], refs[4 + i], sems.at[i]) for i in range(4)]
    for copy in copies:
        copy.start()
    for copy in copies:
        copy.wait()


def body(g, r, tp, queries, keys, values, cotangent, log_sum, chosen, normed_input):
    tok, cols = queries.shape
    bd = tok // BLK
    wide = 2 * tok
    w = normed_input.shape[1] // tp
    vmem = pl.BlockSpec(memory_space=pltpu.VMEM)
    sem = pltpu.SemaphoreType.DMA
    hbm = pl.BlockSpec(memory_space=pltpu.HBM)
    picks = chosen.transpose(2, 0, 1)
    held = [pltpu.VMEM(a.shape, a.dtype) for a in (
        queries, keys, values, cotangent, log_sum, picks, normed_input)]
    made = pl.pallas_call(
        functools.partial(kernel, g, r, tp),
        out_shape=[
            jax.ShapeDtypeStruct((tok, cols), BF16),
            jax.ShapeDtypeStruct((tok, cols), BF16),
            jax.ShapeDtypeStruct((tok, cols), BF16),
            jax.ShapeDtypeStruct((w, cols), F32),
        ],
        in_specs=[hbm] * 7,
        out_specs=[vmem] * 4,
        scratch_shapes=held + [
            sem((7,)),
            pltpu.VMEM((wide, cols), BF16),
            pltpu.VMEM((wide, cols), BF16),
            pltpu.VMEM((r, g, bd, cols), F32),
            pltpu.VMEM((r, g, wide), F32),
            pltpu.VMEM((r, 2, tok, cols), BF16),
            pltpu.VMEM((r, g, 2, BLK, cols), BF16),
            pltpu.VMEM((r * g, 2, BLK, cols), BF16),
            pltpu.VMEM((r, g * BLK, wide), F32),
            pltpu.VMEM((r, g * BLK, wide), F32),
            pltpu.VMEM((2, r, g, BLK, cols), BF16),
            pltpu.VMEM((2, r, g, BLK, cols), BF16),
            pltpu.VMEM((2, r, tok, cols), BF16),
            pltpu.VMEM((2, r, tok, cols), BF16),
            pltpu.VMEM((tok, cols), F32),
            pltpu.VMEM((tok, cols), F32),
            pltpu.VMEM((wide, cols), F32),
            pltpu.VMEM((tp, w, tok), BF16),
            pltpu.VMEM((r, w, tok), BF16),
            pltpu.VMEM((tp, r, w, tok), BF16),
            pltpu.VMEM((r, tok, cols), BF16),
            pltpu.VMEM((g, w, cols), BF16),
            pltpu.VMEM((g, w, cols), BF16),
            sem((2, r)), sem((2, r)),
            sem((r, g)), sem((r, g)),
            sem((2, r, g)), sem((2, r, g)),
            sem((2, r)), sem((2, r)),
            sem((tp,)), sem((r,)),
            sem((tp,)), sem((tp,)),
            sem((r,)), sem((r,)),
            sem((g,)), sem((g,)),
        ],
        compiler_params=pltpu.CompilerParams(
            has_side_effects=True, collective_id=0, vmem_limit_bytes=67043328),
    )(queries, keys, values, cotangent, log_sum, picks, normed_input)
    return pl.pallas_call(
        write_out,
        out_shape=[jax.ShapeDtypeStruct(a.shape, a.dtype) for a in made],
        in_specs=[vmem] * 4,
        out_specs=[hbm] * 4,
        scratch_shapes=[sem((4,))],
    )(*made)


def solution(mesh):
    n, tp = mesh.shape["kv"], mesh.shape["tp"]
    g = n // tp
    in_specs = (
        P("kv", "tp"), P("kv", "tp"), P("kv", "tp"), P("kv", "tp"),
        P("tp", "kv"), P("tp", None, None), P("kv", "tp"),
    )
    out_specs = (P("kv", "tp"),) * 4
    return jax.shard_map(
        functools.partial(body, g, n // g, tp), mesh=mesh, in_specs=in_specs, out_specs=out_specs, check_vma=False
    )
```

```python
import functools

import jax
import jax.numpy as jnp
from jax import lax
from jax.experimental import pallas as pl
from jax.experimental.pallas import tpu as pltpu
from jax.sharding import PartitionSpec as P

HD = 64
BLK = 32
MASKED = -1e30
MESH = pl.DeviceIdType.MESH
F32 = jnp.float32
BF16 = jnp.bfloat16


def dot(a, b, ca, cb):
    return lax.dot_general(a, b, (((ca,), (cb,)), ((), ())), preferred_element_type=F32)


def iota(shape, dim):
    return lax.broadcasted_iota(jnp.int32, shape, dim)


def each(low, high, fn):
    def step(i, carry):
        fn(i)
        return carry
    lax.fori_loop(low, high, step, 0)


def kernel(
    g, r, tp, q_in, k_in, v_in, c_in, lse_in, pick_in, x_in,
    gq_ref, gk_ref, gv_ref, gw_ref,
    q_ref, k_ref, v_ref, c_ref, lse_ref, pick_ref, x_ref, insem,
    qs, cs, hot, bias, kz, kvs, kvt, wts, vds, back_s, back_r, rel_s, rel_r, gko, gvo, dqa,
    xs, xg, xr, dqr, gs, gr, fs, ff, fb, fr,
    zs_sem, zr_sem, ys_sem, yr_sem, bs_sem, br_sem, rs_sem, rr_sem,
    x1s, x1r, x2s, x2r, dqs_sem, dqr_sem, gs_sem, gr_sem,
    fys, fyr, fzs, fzr, fbs, fbr, frs, frr,
):
    tok, cols = q_ref.shape
    sel, heads, blocks = pick_ref.shape
    bd = tok // BLK
    wide = 2 * tok
    chunk = g * BLK
    scale = HD ** (-0.5)
    me, t = lax.axis_index("kv"), lax.axis_index("tp")
    z, y = me // g, lax.rem(me, g)

    def far_of(zz):
        return r - 1 - lax.rem(zz, 4) // 2

    def has_far(zz):
        return (lax.rem(zz, 2) == 0) & (zz < r - 2)

    def is_far(zz, to):
        return has_far(zz) & (far_of(zz) == to)
    far, mine_far = far_of(z), has_far(z)

    loads = {}
    for i, (a, b) in enumerate((
        (pick_in, pick_ref), (k_in, k_ref), (v_in, v_ref), (x_in, x_ref),
        (q_in, q_ref), (c_in, c_ref), (lse_in, lse_ref),
    )):
        loads[i] = pltpu.make_async_copy(a, b, insem.at[i])
        loads[i].start()

    barrier = pltpu.get_barrier_semaphore()

    def greet(kv, tt):
        pl.semaphore_signal(barrier, inc=1, device_id=(kv, tt), device_id_type=MESH)

    for i in range(1, r):
        greet(lax.rem(z + i, r) * g + y, t)
    for i in range(1, g):
        greet(z * g + lax.rem(y + i, g), t)
    for i in range(1, tp):
        greet(me, lax.rem(t + i, tp))
    for i in range(r):
        zz = lax.rem(z + i, r)
        if i == 0:
            @pl.when(t != z)
            def _():
                greet(zz * g + y, z)
        else:
            greet(zz * g + y, z)

    def z_copy(c, zz, slot):
        return pltpu.make_async_remote_copy(
            src_ref=(k_ref, v_ref)[c], dst_ref=kz.at[slot, c], send_sem=zs_sem.at[c, zz],
            recv_sem=zr_sem.at[c, slot], device_id=(zz * g + y, t), device_id_type=MESH)

    def y_copy(zz, yy, slot):
        return pltpu.make_async_remote_copy(
            src_ref=kvs.at[zz, yy], dst_ref=kvt.at[zz * g + slot], send_sem=ys_sem.at[zz, yy],
            recv_sem=yr_sem.at[zz, slot], device_id=(z * g + yy, t), device_id_type=MESH)

    def far_y_copy(yy, slot):
        return pltpu.make_async_remote_copy(
            src_ref=fs.at[yy], dst_ref=ff.at[slot], send_sem=fys.at[yy], recv_sem=fyr.at[slot],
            device_id=(z * g + yy, t), device_id_type=MESH)

    def far_z_copy(slot):
        return pltpu.make_async_remote_copy(
            src_ref=ff, dst_ref=kvt.at[pl.ds(slot * g, g)], send_sem=fzs.at[0], recv_sem=fzr.at[slot],
            device_id=(far * g + y, t), device_id_type=MESH)

    def far_back_copy(c, zz):
        return pltpu.make_async_remote_copy(
            src_ref=back_s.at[c, zz], dst_ref=fb.at[c], send_sem=fbs.at[c, zz], recv_sem=fbr.at[c],
            device_id=(zz * g + y, t), device_id_type=MESH)

    def far_ret_copy(c, yy, slot):
        return pltpu.make_async_remote_copy(
            src_ref=fb.at[c, yy], dst_ref=fr.at[c, slot], send_sem=frs.at[c, yy], recv_sem=frr.at[c, slot],
            device_id=(z * g + yy, t), device_id_type=MESH)

    def back_copy(c, zz, yy, slot):
        return pltpu.make_async_remote_copy(
            src_ref=back_s.at[c, zz, yy], dst_ref=back_r.at[c, zz, slot], send_sem=bs_sem.at[c, zz, yy],
            recv_sem=br_sem.at[c, zz, slot], device_id=(z * g + yy, t), device_id_type=MESH)

    def rel_copy(c, zz, slot):
        return pltpu.make_async_remote_copy(
            src_ref=rel_s.at[c, zz], dst_ref=rel_r.at[c, slot], send_sem=rs_sem.at[c, zz],
            recv_sem=rr_sem.at[c, slot], device_id=(zz * g + y, t), device_id_type=MESH)

    def x1_copy(s, slot):
        return pltpu.make_async_remote_copy(
            src_ref=xs.at[s], dst_ref=xg.at[slot], send_sem=x1s.at[s], recv_sem=x1r.at[slot],
            device_id=(t * g + y, s), device_id_type=MESH)

    def x2_copy(tt, slot):
        return pltpu.make_async_remote_copy(
            src_ref=xg, dst_ref=xr.at[slot], send_sem=x2s.at[tt], recv_sem=x2r.at[slot],
            device_id=(me, tt), device_id_type=MESH)

    def dq_copy(zz, slot):
        return pltpu.make_async_remote_copy(
            src_ref=dqr.at[z], dst_ref=dqr.at[slot], send_sem=dqs_sem.at[zz], recv_sem=dqr_sem.at[slot],
            device_id=(zz * g + y, t), device_id_type=MESH)

    def gw_copy(yy, slot):
        return pltpu.make_async_remote_copy(
            src_ref=gs.at[yy], dst_ref=gr.at[slot], send_sem=gs_sem.at[yy], recv_sem=gr_sem.at[slot],
            device_id=(z * g + yy, t), device_id_type=MESH)

    def each_x1(low, fn):
        def step(s):
            @pl.when((t != z) | (s != t))
            def _():
                fn(s)
        each(low, tp, step)

    def each_x1_in(fn):
        def step(zz):
            @pl.when((t != z) | (zz != z))
            def _():
                fn(zz)
        each(0, r, step)

    loads[0].wait()
    block_of = iota((blocks, heads * g * bd), 0)
    col_of = iota((blocks, heads * g * bd), 1)
    at_row = lax.rem(col_of, g * bd) == block_of - z * (g * bd)
    at_far = lax.rem(col_of, g * bd) == block_of - far * (g * bd)
    at_tok = me * bd + lax.rem(iota((blocks, heads * tok), 1), tok) // BLK == iota((blocks, heads * tok), 0)
    tok_head = iota((blocks, heads * tok), 1) // tok
    row_ids, far_ids, ids = None, None, None
    for h in range(heads):
        mine = pick_ref[:, h, :].astype(F32).astype(BF16)
        pick_row = (at_row & (col_of // (g * bd) == h)).astype(F32).astype(BF16)
        pick_far = (at_far & (col_of // (g * bd) == h)).astype(F32).astype(BF16)
        pick_tok = (at_tok & (tok_head == h)).astype(F32).astype(BF16)
        a, b, f = dot(mine, pick_row, 1, 0), dot(mine, pick_tok, 1, 0), dot(mine, pick_far, 1, 0)
        far_ids = f if far_ids is None else far_ids + f
        row_ids = a if row_ids is None else row_ids + a
        ids = b if ids is None else ids + b
    row_ids = (row_ids + 0.5).astype(jnp.int32)
    far_ids = (far_ids + 0.5).astype(jnp.int32)
    ids = (ids + 0.5).astype(jnp.int32)
    ids = jnp.where(ids < me * bd + lax.rem(iota(ids.shape, 1), tok) // BLK, ids, blocks)
    target_at = iota((r * bd, heads * g * bd), 0)
    target = (target_at // bd * g + y) * bd + lax.rem(target_at, bd)
    hit = jnp.zeros(target.shape, F32)
    own_target = me * bd + iota((2 * bd, heads * g * bd), 0)
    far_hit = jnp.zeros(own_target.shape, F32)
    for s in range(sel):
        hit = jnp.where(row_ids[s : s + 1, :] == target, 1.0, hit)
        far_hit = jnp.where(far_ids[s : s + 1, :] == own_target, 1.0, far_hit)
    out_at, out_from = iota((heads * g * bd, g * cols), 1), iota((heads * g * bd, g * cols), 0)
    fan = (lax.rem(out_from, g * bd) // bd == out_at // cols) & (
        lax.rem(out_at, cols) // HD == out_from // (g * bd))
    fan = fan.astype(F32).astype(BF16)
    far_taken = jnp.where(dot(far_hit.astype(BF16), fan, 1, 0) > 0.5, 1.0, 0.0)
    taken = dot(hit.astype(BF16), fan, 1, 0)
    taken = jnp.where(taken > 0.5, 1.0, 0.0).reshape(r, bd, g * cols)
    for yy in range(g):
        hot[:r, yy] = taken[:, :, yy * cols : (yy + 1) * cols]
        hot[r, yy] = far_taken[:bd, yy * cols : (yy + 1) * cols]

    loads[1].wait()
    loads[2].wait()
    pl.semaphore_wait(barrier, (r - 1) + (g - 1) + (tp - 1) + r - jnp.where(t == z, 1, 0))

    def span(i):
        zz = r - 1 - i

        @pl.when(~is_far(z, zz))
        def _():
            z_copy(0, zz, z).start()
            z_copy(1, zz, z).start()
    each(0, r - 1 - z, span)

    def mask(zz, yy, b):
        return jnp.broadcast_to(hot[zz, yy, pl.ds(b, 1), :], (BLK, cols))

    def picked(zz, yy, k_from, v_from):
        k_out, v_out = None, None
        for b in range(bd):
            one = mask(zz, yy, b).astype(BF16)
            k_term, v_term = k_from(b) * one, v_from(b) * one
            k_out = k_term if k_out is None else k_out + k_term
            v_out = v_term if v_out is None else v_out + v_term
        return k_out, v_out

    def own_picked(zz, yy):
        return picked(zz, yy, lambda b: k_ref[b * BLK : (b + 1) * BLK, :], lambda b: v_ref[b * BLK : (b + 1) * BLK, :])

    @pl.when(mine_far)
    def _():
        def one(k):
            yy = lax.rem(y + k, g)
            a, b = own_picked(r, yy)

            @pl.when(k != g)
            def _():
                fs[yy, 0] = a
                fs[yy, 1] = b
                far_y_copy(yy, y).start()

            @pl.when(k == g)
            def _():
                ff[y, 0] = a
                ff[y, 1] = b
        each(1, g + 1, one)

    def own_rows(i):
        yy = y + 1 + i
        a, b = own_picked(z, yy)
        kvs[z, yy, 0] = a
        kvs[z, yy, 1] = b
        y_copy(z, yy, y).start()
    each(0, g - 1 - y, own_rows)

    loads[3].wait()
    width = x_ref.shape[1]
    w = width // tp
    eye = (iota((width, width), 0) == iota((width, width), 1)).astype(F32).astype(BF16)
    flipped = dot(eye, x_ref[...], 1, 1).astype(BF16)
    xs[...] = flipped.reshape(tp, w, tok)
    each_x1(0, lambda s: x1_copy(s, z).start())

    @pl.when(t == z)
    def _():
        xg[z] = xs[t]

    def clear(yy):
        kvt[z * g + yy] = jnp.zeros(kvt.shape[1:], BF16)
    each(y, g, clear)

    for i in (4, 5, 6):
        loads[i].wait()
    less = jnp.concatenate([-lse_ref[h : h + 1, :] for h in range(heads)], axis=1)
    owner = ids // bd
    for zz in range(r):
        need = jnp.zeros((g, wide), jnp.bool_)
        at = zz * g + iota((g, wide), 0)
        for s in range(sel):
            need = need | (owner[s : s + 1, :] == at)
        bias[zz] = jnp.where(need & (at < me), less, MASKED)
    low = iota((tok, cols), 1) < HD

    def stacked(ref):
        part = ref[...]
        zero = jnp.zeros_like(part)
        return jnp.concatenate([jnp.where(low, part, zero), jnp.where(low, zero, part)], axis=0)

    qs[...] = stacked(q_ref)
    cs[...] = stacked(c_ref)

    @pl.when(mine_far)
    def _():
        for i in range(1, g):
            far_y_copy(0, lax.rem(y + i, g)).wait_recv()
        far_z_copy(z).start()

    key_at = iota((tok, wide), 0)
    query_at = lax.rem(iota((tok, wide), 1), tok)
    own_block = key_at // BLK
    need = jnp.zeros((tok, wide), jnp.bool_)
    own_ids = jnp.where(owner == me, lax.rem(ids, bd), bd)
    for s in range(sel):
        need = need | (own_ids[s : s + 1, :] == own_block)
    need = need | ((own_block == query_at // BLK) & (key_at <= query_at))
    own = jnp.exp(dot(k_ref[...], qs[...], 1, 1) * scale + jnp.where(need, less, MASKED))
    vdo = dot(v_ref[...], cs[...], 1, 1)
    gvo[...] = dot(own.astype(BF16), cs[...], 1, 0)
    first = jnp.sum(own * vdo, axis=0, keepdims=True)

    def relay(i):
        zz = z - 1 - i

        @pl.when(~is_far(zz, z))
        def _():
            z_copy(0, zz, zz).wait_recv()
            z_copy(1, zz, zz).wait_recv()

            def one(k):
                yy = lax.rem(y + k, g)
                a, b = picked(zz, yy, lambda b: kz[zz, 0, b * BLK : (b + 1) * BLK, :],
                              lambda b: kz[zz, 1, b * BLK : (b + 1) * BLK, :])

                @pl.when(k != g)
                def _():
                    kvs[zz, yy, 0] = a
                    kvs[zz, yy, 1] = b
                    y_copy(zz, yy, y).start()

                @pl.when(k == g)
                def _():
                    kvt[zz * g + y, 0] = a
                    kvt[zz * g + y, 1] = b
            each(1, g + 1, one)
    each(0, z, relay)

    each_x1_in(lambda zz: x1_copy(0, zz).wait_recv())
    for i in range(1, tp):
        x2_copy(lax.rem(t + i, tp), t).start()
    xr[t] = xg[...]

    def send_back(c, zz):
        def one(k):
            yy = lax.rem(y + k, g)

            @pl.when((zz < z) | (yy < y))
            def _():
                back_copy(c, zz, yy, y).start()

        @pl.when(is_far(zz, z))
        def _():
            far_back_copy(c, zz).start()

        @pl.when(~is_far(zz, z))
        def _():
            each(1, g, one)

    def pass_one(i, delta):
        zz = z - i

        def arrive(k):
            yy = lax.rem(y + k, g)

            @pl.when((zz < z) | (yy < y))
            def _():
                y_copy(zz, 0, yy).wait_recv()

        @pl.when(is_far(zz, z))
        def _():
            far_z_copy(zz).wait_recv()

        @pl.when(~is_far(zz, z))
        def _():
            each(1, g, arrive)
        kp = kvt[pl.ds(zz * g, g), 0].reshape(chunk, cols)
        vp = kvt[pl.ds(zz * g, g), 1].reshape(chunk, cols)
        line = jnp.concatenate(
            [jnp.broadcast_to(bias[zz, a : a + 1, :], (BLK, wide)) for a in range(g)], axis=0)
        weights = jnp.exp(dot(kp, qs[...], 1, 1) * scale + line)
        vd = dot(vp, cs[...], 1, 1)
        wts[zz] = weights
        vds[zz] = vd
        back_s[1, zz] = dot(weights.astype(BF16), cs[...], 1, 0).astype(BF16).reshape(g, BLK, cols)
        send_back(1, zz)
        return delta + jnp.sum(weights * vd, axis=0, keepdims=True)
    delta = lax.fori_loop(0, z + 1, pass_one, first)

    dso = (own * (vdo - delta)).astype(BF16)
    dqa[...] = dot(dso, k_ref[...], 0, 0)

    def pass_two(i):
        zz = z - i
        kp = kvt[pl.ds(zz * g, g), 0].reshape(chunk, cols)
        ds = (wts[zz] * (vds[zz] - delta)).astype(BF16)
        dqa[...] += dot(ds, kp, 0, 0)
        back_s[0, zz] = (dot(ds, qs[...], 1, 0) * scale).astype(BF16).reshape(g, BLK, cols)
        send_back(0, zz)
    each(0, z + 1, pass_two)

    dq = jnp.where(low, dqa[:tok], dqa[tok:]) * scale
    dq = dq.astype(BF16)
    gq_ref[...] = dq
    dqr[z] = dq
    for i in range(1, r):
        dq_copy(lax.rem(z + i, r), z).start()
    gko[...] = dot(dso, qs[...], 1, 0) * scale

    def relay_back(c):
        own_sum = gko if c == 0 else gvo

        def own_add(i):
            yy = y + 1 + i
            back_copy(c, z, 0, yy).wait_recv()
            got = back_r[c, z, yy].astype(F32)
            for b in range(bd):
                own_sum[b * BLK : (b + 1) * BLK, :] += got * mask(z, yy, b)

        def one(i):
            zz = z - 1 - i

            @pl.when(~is_far(zz, z))
            def _():
                sums = [back_s[c, zz, y].astype(F32) * mask(zz, y, b) for b in range(bd)]

                def add(k, acc):
                    yy = lax.rem(y + k, g)
                    back_copy(c, zz, 0, yy).wait_recv()
                    got = back_r[c, zz, yy].astype(F32)
                    return tuple(acc[b] + got * mask(zz, yy, b) for b in range(bd))
                sums = lax.fori_loop(1, g, add, tuple(sums))
                for b in range(bd):
                    rel_s[c, zz, b * BLK : (b + 1) * BLK, :] = sums[b].astype(BF16)
                rel_copy(c, zz, z).start()
        each(0, z, one)
        each(0, g - 1 - y, own_add)

    def far_forward(c):
        @pl.when(mine_far)
        def _():
            far_back_copy(c, 0).wait_recv()
            for i in range(1, g):
                far_ret_copy(c, lax.rem(y + i, g), y).start()

    def far_add(c):
        own_sum = gko if c == 0 else gvo

        def take(got, yy):
            for b in range(bd):
                own_sum[b * BLK : (b + 1) * BLK, :] += got.astype(F32) * mask(r, yy, b)

        @pl.when(mine_far)
        def _():
            take(fb[c, y], y)

            def one(k):
                yy = lax.rem(y + k, g)
                far_ret_copy(c, 0, yy).wait_recv()
                take(fr[c, yy], yy)
            each(1, g, one)

    relay_back(1)
    far_forward(1)

    for i in range(1, tp):
        tt = lax.rem(t + i, tp)
        x2_copy(tt, tt).wait_recv()
    total = None
    for zz in range(r):
        @pl.when(zz != z)
        def _():
            dq_copy(zz, zz).wait_recv()
        part = dot(xr[:, zz].reshape(width, tok), dqr[zz], 1, 0)
        total = part if total is None else total + part
    for yy in range(g):
        gs[yy] = total[yy * w : (yy + 1) * w].astype(BF16)

        @pl.when(yy == y)
        def _():
            gw_ref[...] = total[yy * w : (yy + 1) * w]
    for i in range(1, g):
        gw_copy(lax.rem(y + i, g), y).start()

    relay_back(0)
    far_forward(0)
    far_add(1)
    far_add(0)

    for i in range(1, g):
        yy = lax.rem(y + i, g)
        gw_copy(yy, yy).wait_recv()
        gw_ref[...] += gr[yy].astype(F32)

    def settle(c):
        own_sum = gko if c == 0 else gvo

        def one(i):
            zz = z + 1 + i

            @pl.when(~is_far(z, zz))
            def _():
                rel_copy(c, 0, zz).wait_recv()
                own_sum[...] += rel_r[c, zz].astype(F32)
        each(0, r - 1 - z, one)
        (gk_ref if c == 0 else gv_ref)[...] = own_sum[...].astype(BF16)
    settle(1)
    settle(0)

    def sent_span(i):
        @pl.when(~is_far(z, z + 1 + i))
        def _():
            z_copy(0, z + 1 + i, z).wait_send()
            z_copy(1, z + 1 + i, z).wait_send()

    @pl.when(mine_far)
    def _():
        far_z_copy(z).wait_send()
        for i in range(1, g):
            yy = lax.rem(y + i, g)
            far_y_copy(yy, y).wait_send()
            far_ret_copy(0, yy, y).wait_send()
            far_ret_copy(1, yy, y).wait_send()
    each(0, r - 1 - z, sent_span)
    each(0, g - 1 - y, lambda i: y_copy(z, y + 1 + i, y).wait_send())

    def sent_row(zz):
        def one(k):
            yy = lax.rem(y + k, g)
            y_copy(zz, yy, y).wait_send()

        @pl.when(~is_far(zz, z))
        def _():
            each(1, g, one)
            rel_copy(0, zz, z).wait_send()
            rel_copy(1, zz, z).wait_send()
    each(0, z, sent_row)

    def sent_back(zz):
        def one(k):
            yy = lax.rem(y + k, g)

            @pl.when((zz < z) | (yy < y))
            def _():
                back_copy(0, zz, yy, y).wait_send()
                back_copy(1, zz, yy, y).wait_send()

        @pl.when(is_far(zz, z))
        def _():
            far_back_copy(0, zz).wait_send()
            far_back_copy(1, zz).wait_send()

        @pl.when(~is_far(zz, z))
        def _():
            each(1, g, one)
    each(0, z + 1, sent_back)
    each_x1(0, lambda s: x1_copy(s, z).wait_send())
    for i in range(1, tp):
        x2_copy(lax.rem(t + i, tp), t).wait_send()
    for i in range(1, r):
        dq_copy(lax.rem(z + i, r), z).wait_send()
    for i in range(1, g):
        gw_copy(lax.rem(y + i, g), y).wait_send()


def write_out(*refs):
    sems = refs[8]
    copies = [pltpu.make_async_copy(refs[i], refs[4 + i], sems.at[i]) for i in range(4)]
    for copy in copies:
        copy.start()
    for copy in copies:
        copy.wait()


def body(g, r, tp, queries, keys, values, cotangent, log_sum, chosen, normed_input):
    tok, cols = queries.shape
    bd = tok // BLK
    wide = 2 * tok
    w = normed_input.shape[1] // tp
    vmem = pl.BlockSpec(memory_space=pltpu.VMEM)
    sem = pltpu.SemaphoreType.DMA
    hbm = pl.BlockSpec(memory_space=pltpu.HBM)
    picks = chosen.transpose(2, 0, 1)
    held = [pltpu.VMEM(a.shape, a.dtype) for a in (
        queries, keys, values, cotangent, log_sum, picks, normed_input)]
    made = pl.pallas_call(
        functools.partial(kernel, g, r, tp),
        out_shape=[
            jax.ShapeDtypeStruct((tok, cols), BF16),
            jax.ShapeDtypeStruct((tok, cols), BF16),
            jax.ShapeDtypeStruct((tok, cols), BF16),
            jax.ShapeDtypeStruct((w, cols), F32),
        ],
        in_specs=[hbm] * 7,
        out_specs=[vmem] * 4,
        scratch_shapes=held + [
            sem((7,)),
            pltpu.VMEM((wide, cols), BF16),
            pltpu.VMEM((wide, cols), BF16),
            pltpu.VMEM((r + 1, g, bd, cols), F32),
            pltpu.VMEM((r, g, wide), F32),
            pltpu.VMEM((r, 2, tok, cols), BF16),
            pltpu.VMEM((r, g, 2, BLK, cols), BF16),
            pltpu.VMEM((r * g, 2, BLK, cols), BF16),
            pltpu.VMEM((r, g * BLK, wide), F32),
            pltpu.VMEM((r, g * BLK, wide), F32),
            pltpu.VMEM((2, r, g, BLK, cols), BF16),
            pltpu.VMEM((2, r, g, BLK, cols), BF16),
            pltpu.VMEM((2, r, tok, cols), BF16),
            pltpu.VMEM((2, r, tok, cols), BF16),
            pltpu.VMEM((tok, cols), F32),
            pltpu.VMEM((tok, cols), F32),
            pltpu.VMEM((wide, cols), F32),
            pltpu.VMEM((tp, w, tok), BF16),
            pltpu.VMEM((r, w, tok), BF16),
            pltpu.VMEM((tp, r, w, tok), BF16),
            pltpu.VMEM((r, tok, cols), BF16),
            pltpu.VMEM((g, w, cols), BF16),
            pltpu.VMEM((g, w, cols), BF16),
            pltpu.VMEM((g, 2, BLK, cols), BF16),
            pltpu.VMEM((g, 2, BLK, cols), BF16),
            pltpu.VMEM((2, g, BLK, cols), BF16),
            pltpu.VMEM((2, g, BLK, cols), BF16),
            sem((2, r)), sem((2, r)),
            sem((r, g)), sem((r, g)),
            sem((2, r, g)), sem((2, r, g)),
            sem((2, r)), sem((2, r)),
            sem((tp,)), sem((r,)),
            sem((tp,)), sem((tp,)),
            sem((r,)), sem((r,)),
            sem((g,)), sem((g,)),
            sem((g,)), sem((g,)),
            sem((1,)), sem((r,)),
            sem((2, r)), sem((2,)),
            sem((2, g)), sem((2, g)),
        ],
        compiler_params=pltpu.CompilerParams(
            has_side_effects=True, collective_id=0, vmem_limit_bytes=67043328),
    )(queries, keys, values, cotangent, log_sum, picks, normed_input)
    return pl.pallas_call(
        write_out,
        out_shape=[jax.ShapeDtypeStruct(a.shape, a.dtype) for a in made],
        in_specs=[vmem] * 4,
        out_specs=[hbm] * 4,
        scratch_shapes=[sem((4,))],
    )(*made)


def solution(mesh):
    n, tp = mesh.shape["kv"], mesh.shape["tp"]
    g = n // tp
    in_specs = (
        P("kv", "tp"), P("kv", "tp"), P("kv", "tp"), P("kv", "tp"),
        P("tp", "kv"), P("tp", None, None), P("kv", "tp"),
    )
    out_specs = (P("kv", "tp"),) * 4
    return jax.shard_map(
        functools.partial(body, g, n // g, tp), mesh=mesh, in_specs=in_specs, out_specs=out_specs, check_vma=False
    )
```

```python
import functools

import jax
import jax.numpy as jnp
from jax import lax
from jax.experimental import pallas as pl
from jax.experimental.pallas import tpu as pltpu
from jax.sharding import PartitionSpec as P

HD = 64
BLK = 32
MASKED = -1e30
MESH = pl.DeviceIdType.MESH
F32 = jnp.float32
BF16 = jnp.bfloat16


def dot(a, b, ca, cb):
    return lax.dot_general(a, b, (((ca,), (cb,)), ((), ())), preferred_element_type=F32)


def iota(shape, dim):
    return lax.broadcasted_iota(jnp.int32, shape, dim)


def each(low, high, fn):
    def step(i, carry):
        fn(i)
        return carry
    lax.fori_loop(low, high, step, 0)


def kernel(
    g, r, tp, q_in, k_in, v_in, c_in, lse_in, pick_in, x_in,
    gq_ref, gk_ref, gv_ref, gw_ref,
    q_ref, kv_ref, c_ref, lse_ref, pick_ref, x_ref, insem,
    qs, cs, hot, bias, kz, kvs, kvt, wts, vds, back_s, back_r, rel_s, rel_r, gko, gvo, dqa,
    xs, xg, xr, dqr, gs, gr, fs, ff, fb, fr,
    zs_sem, zr_sem, ys_sem, yr_sem, bs_sem, br_sem, rs_sem, rr_sem,
    x1s, x1r, x2s, x2r, dqs_sem, dqr_sem, gs_sem, gr_sem,
    fys, fyr, fzs, fzr, fbs, fbr, frs, frr,
):
    k_ref, v_ref = kv_ref.at[0], kv_ref.at[1]
    tok, cols = q_ref.shape
    sel, heads, blocks = pick_ref.shape
    bd = tok // BLK
    wide = 2 * tok
    chunk = g * BLK
    scale = HD ** (-0.5)
    me, t = lax.axis_index("kv"), lax.axis_index("tp")
    z, y = me // g, lax.rem(me, g)

    def far_of(zz):
        return r - 1 - lax.rem(zz, 4) // 2

    def has_far(zz):
        return (lax.rem(zz, 2) == 0) & (zz < r - 2)

    def is_far(zz, to):
        return has_far(zz) & (far_of(zz) == to)
    far, mine_far = far_of(z), has_far(z)

    loads = {}
    for i, (a, b) in enumerate((
        (pick_in, pick_ref), (k_in, k_ref), (v_in, v_ref), (x_in, x_ref),
        (q_in, q_ref), (c_in, c_ref), (lse_in, lse_ref),
    )):
        loads[i] = pltpu.make_async_copy(a, b, insem.at[i])
        loads[i].start()

    barrier = pltpu.get_barrier_semaphore()

    def greet(kv, tt):
        pl.semaphore_signal(barrier, inc=1, device_id=(kv, tt), device_id_type=MESH)

    for i in range(1, r):
        greet(lax.rem(z + i, r) * g + y, t)
    for i in range(1, g):
        greet(z * g + lax.rem(y + i, g), t)
    for i in range(1, tp):
        greet(me, lax.rem(t + i, tp))
    for i in range(r):
        zz = lax.rem(z + i, r)
        if i == 0:
            @pl.when(t != z)
            def _():
                greet(zz * g + y, z)
        else:
            greet(zz * g + y, z)

    def remote(src, dst, ssem, rsem, kv, tt):
        return pltpu.make_async_remote_copy(
            src_ref=src, dst_ref=dst, send_sem=ssem, recv_sem=rsem, device_id=(kv, tt), device_id_type=MESH)

    def z_copy(zz, slot):
        return remote(kv_ref, kz.at[slot], zs_sem.at[0], zr_sem.at[slot], zz * g + y, t)

    def y_copy(zz, yy, slot):
        return remote(kvs.at[zz, yy], kvt.at[zz * g + slot], ys_sem.at[zz], yr_sem.at[zz], z * g + yy, t)

    def far_y_copy(yy, slot):
        return remote(fs.at[yy], ff.at[slot], fys.at[0], fyr.at[0], z * g + yy, t)

    def far_z_copy(slot):
        return remote(ff, kvt.at[pl.ds(slot * g, g)], fzs.at[0], fzr.at[slot // 4], far * g + y, t)

    def far_back_copy(c, zz):
        return remote(back_s.at[c, zz], fb.at[c], fbs.at[c, zz // 4], fbr.at[c], zz * g + y, t)

    def far_ret_copy(c, yy, slot):
        return remote(fb.at[c, yy], fr.at[c, slot], frs.at[c], frr.at[c], z * g + yy, t)

    def back_copy(c, zz, yy, slot):
        return remote(back_s.at[c, zz, yy], back_r.at[c, zz, slot], bs_sem.at[c, zz], br_sem.at[c, zz], z * g + yy, t)

    def rel_copy(c, zz, slot):
        return remote(rel_s.at[c, zz], rel_r.at[c, slot], rs_sem.at[c], rr_sem.at[c, slot], zz * g + y, t)

    def x1_copy(s, slot):
        return remote(xs.at[s], xg.at[slot], x1s.at[0], x1r.at[0], t * g + y, s)

    def x2_copy(tt, slot):
        return remote(xg, xr.at[slot], x2s.at[0], x2r.at[0], me, tt)

    def dq_copy(zz, slot):
        return remote(dqr.at[z], dqr.at[slot], dqs_sem.at[0], dqr_sem.at[0], zz * g + y, t)

    def gw_copy(yy, slot):
        return remote(gs.at[yy], gr.at[slot], gs_sem.at[0], gr_sem.at[0], z * g + yy, t)

    other = z * g + lax.rem(y + 1, g)

    def arrived(ref, sem):
        remote(ref, ref, sem, sem, other, t).wait_recv()

    def left(ref, sem):
        remote(ref, ref, sem, sem, other, t).wait_send()

    def counted(count, most, fn):
        for i in range(1, most + 1):
            @pl.when(count == i)
            def _():
                fn(i)

    def each_x1(low, fn):
        def step(s):
            @pl.when((t != z) | (s != t))
            def _():
                fn(s)
        each(low, tp, step)

    loads[0].wait()
    block_of = iota((blocks, heads * g * bd), 0)
    col_of = iota((blocks, heads * g * bd), 1)
    at_row = lax.rem(col_of, g * bd) == block_of - z * (g * bd)
    at_far = lax.rem(col_of, g * bd) == block_of - far * (g * bd)
    at_tok = me * bd + lax.rem(iota((blocks, heads * tok), 1), tok) // BLK == iota((blocks, heads * tok), 0)
    tok_head = iota((blocks, heads * tok), 1) // tok
    row_ids, far_ids, ids = None, None, None
    for h in range(heads):
        mine = pick_ref[:, h, :].astype(F32).astype(BF16)
        pick_row = (at_row & (col_of // (g * bd) == h)).astype(F32).astype(BF16)
        pick_far = (at_far & (col_of // (g * bd) == h)).astype(F32).astype(BF16)
        pick_tok = (at_tok & (tok_head == h)).astype(F32).astype(BF16)
        a, b, f = dot(mine, pick_row, 1, 0), dot(mine, pick_tok, 1, 0), dot(mine, pick_far, 1, 0)
        far_ids = f if far_ids is None else far_ids + f
        row_ids = a if row_ids is None else row_ids + a
        ids = b if ids is None else ids + b
    row_ids = (row_ids + 0.5).astype(jnp.int32)
    far_ids = (far_ids + 0.5).astype(jnp.int32)
    ids = (ids + 0.5).astype(jnp.int32)
    ids = jnp.where(ids < me * bd + lax.rem(iota(ids.shape, 1), tok) // BLK, ids, blocks)
    target_at = iota((r * bd, heads * g * bd), 0)
    target = (target_at // bd * g + y) * bd + lax.rem(target_at, bd)
    hit = jnp.zeros(target.shape, F32)
    own_target = me * bd + iota((2 * bd, heads * g * bd), 0)
    far_hit = jnp.zeros(own_target.shape, F32)
    for s in range(sel):
        hit = jnp.where(row_ids[s : s + 1, :] == target, 1.0, hit)
        far_hit = jnp.where(far_ids[s : s + 1, :] == own_target, 1.0, far_hit)
    out_at, out_from = iota((heads * g * bd, g * cols), 1), iota((heads * g * bd, g * cols), 0)
    fan = (lax.rem(out_from, g * bd) // bd == out_at // cols) & (
        lax.rem(out_at, cols) // HD == out_from // (g * bd))
    fan = fan.astype(F32).astype(BF16)
    far_taken = jnp.where(dot(far_hit.astype(BF16), fan, 1, 0) > 0.5, 1.0, 0.0)
    taken = dot(hit.astype(BF16), fan, 1, 0)
    taken = jnp.where(taken > 0.5, 1.0, 0.0).reshape(r, bd, g * cols)
    for yy in range(g):
        hot[:r, yy] = taken[:, :, yy * cols : (yy + 1) * cols]
        hot[r, yy] = far_taken[:bd, yy * cols : (yy + 1) * cols]

    loads[1].wait()
    loads[2].wait()
    pl.semaphore_wait(barrier, (r - 1) + (g - 1) + (tp - 1) + r - jnp.where(t == z, 1, 0))

    def span(i):
        zz = r - 1 - i

        @pl.when(~is_far(z, zz))
        def _():
            z_copy(zz, z).start()
    each(0, r - 1 - z, span)

    def mask(zz, yy, b):
        return jnp.broadcast_to(hot[zz, yy, pl.ds(b, 1), :], (BLK, cols))

    def picked(zz, yy, k_from, v_from):
        k_out, v_out = None, None
        for b in range(bd):
            one = mask(zz, yy, b).astype(BF16)
            k_term, v_term = k_from(b) * one, v_from(b) * one
            k_out = k_term if k_out is None else k_out + k_term
            v_out = v_term if v_out is None else v_out + v_term
        return k_out, v_out

    def own_picked(zz, yy):
        return picked(zz, yy, lambda b: k_ref[b * BLK : (b + 1) * BLK, :], lambda b: v_ref[b * BLK : (b + 1) * BLK, :])

    @pl.when(mine_far)
    def _():
        def one(k):
            yy = lax.rem(y + k, g)
            a, b = own_picked(r, yy)

            @pl.when(k != g)
            def _():
                fs[yy, 0] = a
                fs[yy, 1] = b
                far_y_copy(yy, y).start()

            @pl.when(k == g)
            def _():
                ff[y, 0] = a
                ff[y, 1] = b
        each(1, g + 1, one)

    def own_rows(i):
        yy = y + 1 + i
        a, b = own_picked(z, yy)
        kvs[z, yy, 0] = a
        kvs[z, yy, 1] = b
        y_copy(z, yy, y).start()
    each(0, g - 1 - y, own_rows)

    loads[3].wait()
    width = x_ref.shape[1]
    w = width // tp
    eye = (iota((width, width), 0) == iota((width, width), 1)).astype(F32).astype(BF16)
    flipped = dot(eye, x_ref[...], 1, 1).astype(BF16)
    xs[...] = flipped.reshape(tp, w, tok)
    each_x1(0, lambda s: x1_copy(s, z).start())

    @pl.when(t == z)
    def _():
        xg[z] = xs[t]

    def clear(yy):
        kvt[z * g + yy] = jnp.zeros(kvt.shape[1:], BF16)
    each(y, g, clear)

    for i in (4, 5, 6):
        loads[i].wait()
    less = jnp.concatenate([-lse_ref[h : h + 1, :] for h in range(heads)], axis=1)
    owner = ids // bd
    for zz in range(r):
        need = jnp.zeros((g, wide), jnp.bool_)
        at = zz * g + iota((g, wide), 0)
        for s in range(sel):
            need = need | (owner[s : s + 1, :] == at)
        bias[zz] = jnp.where(need & (at < me), less, MASKED)
    low = iota((tok, cols), 1) < HD

    def stacked(ref):
        part = ref[...]
        zero = jnp.zeros_like(part)
        return jnp.concatenate([jnp.where(low, part, zero), jnp.where(low, zero, part)], axis=0)

    qs[...] = stacked(q_ref)
    cs[...] = stacked(c_ref)

    key_at = iota((tok, wide), 0)
    query_at = lax.rem(iota((tok, wide), 1), tok)
    own_block = key_at // BLK
    need = jnp.zeros((tok, wide), jnp.bool_)
    own_ids = jnp.where(owner == me, lax.rem(ids, bd), bd)
    for s in range(sel):
        need = need | (own_ids[s : s + 1, :] == own_block)
    need = need | ((own_block == query_at // BLK) & (key_at <= query_at))
    own = jnp.exp(dot(k_ref[...], qs[...], 1, 1) * scale + jnp.where(need, less, MASKED))
    vdo = dot(v_ref[...], cs[...], 1, 1)
    gvo[...] = dot(own.astype(BF16), cs[...], 1, 0)
    first = jnp.sum(own * vdo, axis=0, keepdims=True)

    def relay(i):
        zz = z - 1 - i

        @pl.when(~is_far(zz, z))
        def _():
            z_copy(zz, zz).wait_recv()

            def one(k):
                yy = lax.rem(y + k, g)
                a, b = picked(zz, yy, lambda b: kz[zz, 0, b * BLK : (b + 1) * BLK, :],
                              lambda b: kz[zz, 1, b * BLK : (b + 1) * BLK, :])

                @pl.when(k != g)
                def _():
                    kvs[zz, yy, 0] = a
                    kvs[zz, yy, 1] = b
                    y_copy(zz, yy, y).start()

                @pl.when(k == g)
                def _():
                    kvt[zz * g + y, 0] = a
                    kvt[zz * g + y, 1] = b
            each(1, g + 1, one)
    once = jnp.minimum(z, 1)
    each(0, once, relay)

    @pl.when(mine_far)
    def _():
        arrived(ff.at[pl.ds(0, g - 1)], fyr.at[0])
        far_z_copy(z).start()
    each(once, z, relay)

    def send_back(c, zz):
        def one(k):
            yy = lax.rem(y + k, g)

            @pl.when((zz < z) | (yy < y))
            def _():
                back_copy(c, zz, yy, y).start()

        @pl.when(is_far(zz, z))
        def _():
            far_back_copy(c, zz).start()

        @pl.when(~is_far(zz, z))
        def _():
            each(1, g, one)

    def pass_one(i, delta):
        zz = z - i

        @pl.when(is_far(zz, z))
        def _():
            far_z_copy(zz).wait_recv()

        @pl.when((zz < z) & ~is_far(zz, z))
        def _():
            arrived(kvt.at[pl.ds(zz * g, g - 1)], yr_sem.at[zz])

        @pl.when(zz == z)
        def _():
            counted(y, g - 1, lambda i: arrived(kvt.at[pl.ds(z * g, i)], yr_sem.at[z]))
        kp = kvt[pl.ds(zz * g, g), 0].reshape(chunk, cols)
        vp = kvt[pl.ds(zz * g, g), 1].reshape(chunk, cols)
        line = jnp.concatenate(
            [jnp.broadcast_to(bias[zz, a : a + 1, :], (BLK, wide)) for a in range(g)], axis=0)
        weights = jnp.exp(dot(kp, qs[...], 1, 1) * scale + line)
        vd = dot(vp, cs[...], 1, 1)
        wts[zz] = weights
        vds[zz] = vd
        back_s[1, zz] = dot(weights.astype(BF16), cs[...], 1, 0).astype(BF16).reshape(g, BLK, cols)
        send_back(1, zz)
        return delta + jnp.sum(weights * vd, axis=0, keepdims=True)
    delta = lax.fori_loop(0, z + 1, pass_one, first)

    dso = (own * (vdo - delta)).astype(BF16)
    dqa[...] = dot(dso, k_ref[...], 0, 0)

    def pass_two(i):
        zz = z - i
        kp = kvt[pl.ds(zz * g, g), 0].reshape(chunk, cols)
        ds = (wts[zz] * (vds[zz] - delta)).astype(BF16)
        dqa[...] += dot(ds, kp, 0, 0)
        back_s[0, zz] = (dot(ds, qs[...], 1, 0) * scale).astype(BF16).reshape(g, BLK, cols)
        send_back(0, zz)
    each(0, z + 1, pass_two)

    dq = jnp.where(low, dqa[:tok], dqa[tok:]) * scale
    dq = dq.astype(BF16)
    gq_ref[...] = dq
    dqr[z] = dq
    for i in range(1, r):
        dq_copy(lax.rem(z + i, r), z).start()
    gko[...] = dot(dso, qs[...], 1, 0) * scale

    counted(tp - jnp.where(t == z, 1, 0), tp, lambda i: arrived(xg.at[pl.ds(0, i)], x1r.at[0]))
    for i in range(1, tp):
        x2_copy(lax.rem(t + i, tp), t).start()
    xr[t] = xg[...]

    def relay_back(c):
        own_sum = gko if c == 0 else gvo

        def own_add(i):
            yy = y + 1 + i
            got = back_r[c, z, yy].astype(F32)
            for b in range(bd):
                own_sum[b * BLK : (b + 1) * BLK, :] += got * mask(z, yy, b)

        def one(i):
            zz = z - 1 - i

            @pl.when(~is_far(zz, z))
            def _():
                arrived(back_r.at[c, zz, pl.ds(0, g - 1)], br_sem.at[c, zz])
                sums = [back_s[c, zz, y].astype(F32) * mask(zz, y, b) for b in range(bd)]

                def add(k, acc):
                    yy = lax.rem(y + k, g)
                    got = back_r[c, zz, yy].astype(F32)
                    return tuple(acc[b] + got * mask(zz, yy, b) for b in range(bd))
                sums = lax.fori_loop(1, g, add, tuple(sums))
                for b in range(bd):
                    rel_s[c, zz, b * BLK : (b + 1) * BLK, :] = sums[b].astype(BF16)
                rel_copy(c, zz, z).start()
        each(0, z, one)
        counted(g - 1 - y, g - 1, lambda i: arrived(back_r.at[c, z, pl.ds(0, i)], br_sem.at[c, z]))
        each(0, g - 1 - y, own_add)

    def far_forward(c):
        @pl.when(mine_far)
        def _():
            far_back_copy(c, 0).wait_recv()
            for i in range(1, g):
                far_ret_copy(c, lax.rem(y + i, g), y).start()

    def far_add(c):
        own_sum = gko if c == 0 else gvo

        def take(got, yy):
            for b in range(bd):
                own_sum[b * BLK : (b + 1) * BLK, :] += got.astype(F32) * mask(r, yy, b)

        @pl.when(mine_far)
        def _():
            take(fb[c, y], y)
            arrived(fr.at[c, pl.ds(0, g - 1)], frr.at[c])

            def one(k):
                yy = lax.rem(y + k, g)
                take(fr[c, yy], yy)
            each(1, g, one)

    relay_back(1)
    far_forward(1)
    far_forward(0)

    arrived(xr.at[pl.ds(0, tp - 1)], x2r.at[0])
    arrived(dqr.at[pl.ds(0, r - 1)], dqr_sem.at[0])
    total = None
    for zz in range(r):
        part = dot(xr[:, zz].reshape(width, tok), dqr[zz], 1, 0)
        total = part if total is None else total + part
    for yy in range(g):
        gs[yy] = total[yy * w : (yy + 1) * w].astype(BF16)

        @pl.when(yy == y)
        def _():
            gw_ref[...] = total[yy * w : (yy + 1) * w]
    for i in range(1, g):
        gw_copy(lax.rem(y + i, g), y).start()

    relay_back(0)
    far_add(1)
    far_add(0)

    arrived(gr.at[pl.ds(0, g - 1)], gr_sem.at[0])
    for i in range(1, g):
        gw_ref[...] += gr[lax.rem(y + i, g)].astype(F32)

    def settle(c):
        own_sum = gko if c == 0 else gvo

        def one(i):
            zz = z + 1 + i

            @pl.when(~is_far(z, zz))
            def _():
                rel_copy(c, 0, zz).wait_recv()
                own_sum[...] += rel_r[c, zz].astype(F32)
        each(0, r - 1 - z, one)
        (gk_ref if c == 0 else gv_ref)[...] = own_sum[...].astype(BF16)
    settle(1)
    settle(0)

    in_far = jnp.where(z == r - 1, 2, 0) + jnp.where(z == r - 2, 1, 0)
    counted(r - 1 - z - jnp.where(mine_far, 1, 0), r - 1, lambda i: left(kz.at[pl.ds(0, i)], zs_sem.at[0]))
    counted(g - 1 - y, g - 1, lambda i: left(kvs.at[z, pl.ds(0, i)], ys_sem.at[z]))

    @pl.when(mine_far)
    def _():
        far_z_copy(z).wait_send()
        left(fs.at[pl.ds(0, g - 1)], fys.at[0])
        left(fb.at[0, pl.ds(0, g - 1)], frs.at[0])
        left(fb.at[1, pl.ds(0, g - 1)], frs.at[1])

    for c in range(2):
        counted(z - in_far, r - 1, lambda i: left(rel_s.at[c, pl.ds(0, i)], rs_sem.at[c]))
        counted(y, g - 1, lambda i: left(back_s.at[c, z, pl.ds(0, i)], bs_sem.at[c, z]))

    def sent_row(zz):
        @pl.when(is_far(zz, z))
        def _():
            far_back_copy(0, zz).wait_send()
            far_back_copy(1, zz).wait_send()

        @pl.when(~is_far(zz, z))
        def _():
            left(kvs.at[zz, pl.ds(0, g - 1)], ys_sem.at[zz])
            left(back_s.at[0, zz, pl.ds(0, g - 1)], bs_sem.at[0, zz])
            left(back_s.at[1, zz, pl.ds(0, g - 1)], bs_sem.at[1, zz])
    each(0, z, sent_row)
    counted(tp - jnp.where(t == z, 1, 0), tp, lambda i: left(xs.at[pl.ds(0, i)], x1s.at[0]))
    left(xr.at[pl.ds(0, tp - 1)], x2s.at[0])
    left(dqr.at[pl.ds(0, r - 1)], dqs_sem.at[0])
    left(gs.at[pl.ds(0, g - 1)], gs_sem.at[0])


def write_out(*refs):
    sems = refs[8]
    copies = [pltpu.make_async_copy(refs[i], refs[4 + i], sems.at[i]) for i in range(4)]
    for copy in copies:
        copy.start()
    for copy in copies:
        copy.wait()


def body(g, r, tp, queries, keys, values, cotangent, log_sum, chosen, normed_input):
    tok, cols = queries.shape
    bd = tok // BLK
    wide = 2 * tok
    w = normed_input.shape[1] // tp
    vmem = pl.BlockSpec(memory_space=pltpu.VMEM)
    sem = pltpu.SemaphoreType.DMA
    hbm = pl.BlockSpec(memory_space=pltpu.HBM)
    picks = chosen.transpose(2, 0, 1)
    held = [pltpu.VMEM(a.shape, a.dtype) for a in (
        queries, jax.ShapeDtypeStruct((2, tok, cols), BF16), cotangent, log_sum, picks, normed_input)]
    made = pl.pallas_call(
        functools.partial(kernel, g, r, tp),
        out_shape=[
            jax.ShapeDtypeStruct((tok, cols), BF16),
            jax.ShapeDtypeStruct((tok, cols), BF16),
            jax.ShapeDtypeStruct((tok, cols), BF16),
            jax.ShapeDtypeStruct((w, cols), F32),
        ],
        in_specs=[hbm] * 7,
        out_specs=[vmem] * 4,
        scratch_shapes=held + [
            sem((7,)),
            pltpu.VMEM((wide, cols), BF16),
            pltpu.VMEM((wide, cols), BF16),
            pltpu.VMEM((r + 1, g, bd, cols), F32),
            pltpu.VMEM((r, g, wide), F32),
            pltpu.VMEM((r, 2, tok, cols), BF16),
            pltpu.VMEM((r, g, 2, BLK, cols), BF16),
            pltpu.VMEM((r * g, 2, BLK, cols), BF16),
            pltpu.VMEM((r, g * BLK, wide), F32),
            pltpu.VMEM((r, g * BLK, wide), F32),
            pltpu.VMEM((2, r, g, BLK, cols), BF16),
            pltpu.VMEM((2, r, g, BLK, cols), BF16),
            pltpu.VMEM((2, r, tok, cols), BF16),
            pltpu.VMEM((2, r, tok, cols), BF16),
            pltpu.VMEM((tok, cols), F32),
            pltpu.VMEM((tok, cols), F32),
            pltpu.VMEM((wide, cols), F32),
            pltpu.VMEM((tp, w, tok), BF16),
            pltpu.VMEM((r, w, tok), BF16),
            pltpu.VMEM((tp, r, w, tok), BF16),
            pltpu.VMEM((r, tok, cols), BF16),
            pltpu.VMEM((g, w, cols), BF16),
            pltpu.VMEM((g, w, cols), BF16),
            pltpu.VMEM((g, 2, BLK, cols), BF16),
            pltpu.VMEM((g, 2, BLK, cols), BF16),
            pltpu.VMEM((2, g, BLK, cols), BF16),
            pltpu.VMEM((2, g, BLK, cols), BF16),
            sem((1,)), sem((r,)),
            sem((r,)), sem((r,)),
            sem((2, r)), sem((2, r)),
            sem((2,)), sem((2, r)),
            sem((1,)), sem((1,)),
            sem((1,)), sem((1,)),
            sem((1,)), sem((1,)),
            sem((1,)), sem((1,)),
            sem((1,)), sem((1,)),
            sem((1,)), sem((2,)),
            sem((2, 2)), sem((2,)),
            sem((2,)), sem((2,)),
        ],
        compiler_params=pltpu.CompilerParams(
            has_side_effects=True, collective_id=0, vmem_limit_bytes=67043328),
    )(queries, keys, values, cotangent, log_sum, picks, normed_input)
    return pl.pallas_call(
        write_out,
        out_shape=[jax.ShapeDtypeStruct(a.shape, a.dtype) for a in made],
        in_specs=[vmem] * 4,
        out_specs=[hbm] * 4,
        scratch_shapes=[sem((4,))],
    )(*made)


def solution(mesh):
    n, tp = mesh.shape["kv"], mesh.shape["tp"]
    g = n // tp
    in_specs = (
        P("kv", "tp"), P("kv", "tp"), P("kv", "tp"), P("kv", "tp"),
        P("tp", "kv"), P("tp", None, None), P("kv", "tp"),
    )
    out_specs = (P("kv", "tp"),) * 4
    return jax.shard_map(
        functools.partial(body, g, n // g, tp), mesh=mesh, in_specs=in_specs, out_specs=out_specs, check_vma=False
    )
```

```python
import functools

import jax
import jax.numpy as jnp
from jax import lax
from jax.experimental import pallas as pl
from jax.experimental.pallas import tpu as pltpu
from jax.sharding import PartitionSpec as P

HD = 64
BLK = 32
MASKED = -1e30
MESH = pl.DeviceIdType.MESH
F32 = jnp.float32
BF16 = jnp.bfloat16


def dot(a, b, ca, cb):
    return lax.dot_general(a, b, (((ca,), (cb,)), ((), ())), preferred_element_type=F32)


def iota(shape, dim):
    return lax.broadcasted_iota(jnp.int32, shape, dim)


def each(low, high, fn):
    def step(i, carry):
        fn(i)
        return carry
    lax.fori_loop(low, high, step, 0)


def far_first(n):
    return sorted(range(1, n), key=lambda i: -min(i, n - i))


def kernel(
    g, r, tp, q_in, k_in, v_in, c_in, lse_in, pick_in, x_in,
    gq_ref, gk_ref, gv_ref, gw_ref,
    q_ref, kv_ref, c_ref, lse_ref, pick_ref, x_ref, insem,
    qs, cs, hot, bias, kz, kvs, kvt, wts, vds, dss, back_s, back_r, rel_s, rel_r, gko, gvo, dqa,
    xs, xg, xr, dqr, gs, gr, fs, ff, fb, fr,
    zs_sem, zr_sem, ys_sem, yr_sem, bs_sem, br_sem, rs_sem, rr_sem,
    x1s, x1r, x2s, x2r, dqs_sem, dqr_sem, gs_sem, gr_sem,
    fys, fyr, fzs, fzr, fbs, fbr, frs, frr,
):
    k_ref, v_ref = kv_ref.at[0], kv_ref.at[1]
    tok, cols = q_ref.shape
    sel, heads, blocks = pick_ref.shape
    bd = tok // BLK
    wide = 2 * tok
    chunk = g * BLK
    scale = HD ** (-0.5)
    me, t = lax.axis_index("kv"), lax.axis_index("tp")
    z, y = me // g, lax.rem(me, g)

    def far_of(zz):
        return r - 1 - lax.rem(zz, 4) // 2

    def has_far(zz):
        return (lax.rem(zz, 2) == 0) & (zz < r - 2)

    def is_far(zz, to):
        return has_far(zz) & (far_of(zz) == to)

    def far_back(zz):
        return (zz == 2) | (zz == 4)

    def is_far_back(zz, to):
        return far_back(zz) & (far_of(zz) == to)
    far, mine_far, mine_far_back = far_of(z), has_far(z), far_back(z)

    loads = {}
    for i, (a, b) in enumerate((
        (pick_in, pick_ref), (k_in, k_ref), (v_in, v_ref), (x_in, x_ref),
        (q_in, q_ref), (c_in, c_ref), (lse_in, lse_ref),
    )):
        loads[i] = pltpu.make_async_copy(a, b, insem.at[i])
        loads[i].start()

    barrier = pltpu.get_barrier_semaphore()

    def greet(kv, tt):
        pl.semaphore_signal(barrier, inc=1, device_id=(kv, tt), device_id_type=MESH)

    for i in range(1, r):
        greet(lax.rem(z + i, r) * g + y, t)
    for i in range(1, g):
        greet(z * g + lax.rem(y + i, g), t)
    for i in range(1, tp):
        greet(me, lax.rem(t + i, tp))
    for i in range(r):
        zz = lax.rem(z + i, r)
        if i == 0:
            @pl.when(t != z)
            def _():
                greet(zz * g + y, z)
        else:
            greet(zz * g + y, z)

    def remote(src, dst, ssem, rsem, kv, tt):
        return pltpu.make_async_remote_copy(
            src_ref=src, dst_ref=dst, send_sem=ssem, recv_sem=rsem, device_id=(kv, tt), device_id_type=MESH)

    def z_copy(zz, slot):
        return remote(kv_ref, kz.at[slot], zs_sem.at[0], zr_sem.at[slot], zz * g + y, t)

    def y_copy(zz, yy, slot):
        return remote(kvs.at[zz, yy], kvt.at[zz * g + slot], ys_sem.at[zz], yr_sem.at[zz], z * g + yy, t)

    def far_y_copy(yy, slot):
        return remote(fs.at[yy], ff.at[slot], fys.at[0], fyr.at[0], z * g + yy, t)

    def far_z_copy(slot):
        return remote(ff, kvt.at[pl.ds(slot * g, g)], fzs.at[0], fzr.at[slot // 4], far * g + y, t)

    def far_back_copy(c, zz):
        return remote(back_s.at[c, zz], fb.at[c], fbs.at[c, zz // 4], fbr.at[c], zz * g + y, t)

    def far_ret_copy(c, yy, slot):
        return remote(fb.at[c, yy], fr.at[c, slot], frs.at[c], frr.at[c], z * g + yy, t)

    def back_copy(c, zz, yy, slot):
        return remote(back_s.at[c, zz, yy], back_r.at[c, zz, slot], bs_sem.at[c, zz], br_sem.at[c, zz], z * g + yy, t)

    def rel_copy(c, zz, slot):
        return remote(rel_s.at[c, zz], rel_r.at[c, slot], rs_sem.at[c], rr_sem.at[c, slot], zz * g + y, t)

    def x1_copy(s, slot):
        return remote(xs.at[s], xg.at[slot], x1s.at[0], x1r.at[0], t * g + y, s)

    def x2_copy(tt, slot):
        return remote(xg, xr.at[slot], x2s.at[0], x2r.at[0], me, tt)

    def dq_copy(zz, slot):
        return remote(dqr.at[z], dqr.at[slot], dqs_sem.at[0], dqr_sem.at[0], zz * g + y, t)

    def gw_copy(yy, slot):
        return remote(gs.at[yy], gr.at[slot], gs_sem.at[0], gr_sem.at[0], z * g + yy, t)

    other = z * g + lax.rem(y + 1, g)

    def arrived(ref, sem):
        remote(ref, ref, sem, sem, other, t).wait_recv()

    def left(ref, sem):
        remote(ref, ref, sem, sem, other, t).wait_send()

    def counted(count, most, fn):
        for i in range(1, most + 1):
            @pl.when(count == i)
            def _():
                fn(i)

    def each_x1(low, fn):
        def step(s):
            @pl.when((t != z) | (s != t))
            def _():
                fn(s)
        each(low, tp, step)

    loads[0].wait()
    block_of = iota((blocks, heads * g * bd), 0)
    col_of = iota((blocks, heads * g * bd), 1)
    at_row = lax.rem(col_of, g * bd) == block_of - z * (g * bd)
    at_far = lax.rem(col_of, g * bd) == block_of - far * (g * bd)
    at_tok = me * bd + lax.rem(iota((blocks, heads * tok), 1), tok) // BLK == iota((blocks, heads * tok), 0)
    tok_head = iota((blocks, heads * tok), 1) // tok
    row_ids, far_ids, ids = None, None, None
    for h in range(heads):
        mine = pick_ref[:, h, :].astype(F32).astype(BF16)
        pick_row = (at_row & (col_of // (g * bd) == h)).astype(F32).astype(BF16)
        pick_far = (at_far & (col_of // (g * bd) == h)).astype(F32).astype(BF16)
        pick_tok = (at_tok & (tok_head == h)).astype(F32).astype(BF16)
        a, b, f = dot(mine, pick_row, 1, 0), dot(mine, pick_tok, 1, 0), dot(mine, pick_far, 1, 0)
        far_ids = f if far_ids is None else far_ids + f
        row_ids = a if row_ids is None else row_ids + a
        ids = b if ids is None else ids + b
    row_ids = (row_ids + 0.5).astype(jnp.int32)
    far_ids = (far_ids + 0.5).astype(jnp.int32)
    ids = (ids + 0.5).astype(jnp.int32)
    ids = jnp.where(ids < me * bd + lax.rem(iota(ids.shape, 1), tok) // BLK, ids, blocks)
    target_at = iota((r * bd, heads * g * bd), 0)
    target = (target_at // bd * g + y) * bd + lax.rem(target_at, bd)
    hit = jnp.zeros(target.shape, F32)
    own_target = me * bd + iota((2 * bd, heads * g * bd), 0)
    far_hit = jnp.zeros(own_target.shape, F32)
    for s in range(sel):
        hit = jnp.where(row_ids[s : s + 1, :] == target, 1.0, hit)
        far_hit = jnp.where(far_ids[s : s + 1, :] == own_target, 1.0, far_hit)
    out_at, out_from = iota((heads * g * bd, g * cols), 1), iota((heads * g * bd, g * cols), 0)
    fan = (lax.rem(out_from, g * bd) // bd == out_at // cols) & (
        lax.rem(out_at, cols) // HD == out_from // (g * bd))
    fan = fan.astype(F32).astype(BF16)
    far_taken = jnp.where(dot(far_hit.astype(BF16), fan, 1, 0) > 0.5, 1.0, 0.0)
    taken = dot(hit.astype(BF16), fan, 1, 0)
    taken = jnp.where(taken > 0.5, 1.0, 0.0).reshape(r, bd, g * cols)
    for yy in range(g):
        hot[:r, yy] = taken[:, :, yy * cols : (yy + 1) * cols]
        hot[r, yy] = far_taken[:bd, yy * cols : (yy + 1) * cols]

    loads[1].wait()
    loads[2].wait()
    pl.semaphore_wait(barrier, (r - 1) + (g - 1) + (tp - 1) + r - jnp.where(t == z, 1, 0))

    def span(i):
        zz = z + 1 + i

        @pl.when(~is_far(z, zz))
        def _():
            z_copy(zz, z).start()
    each(0, r - 1 - z, span)

    def mask(zz, yy, b):
        return jnp.broadcast_to(hot[zz, yy, pl.ds(b, 1), :], (BLK, cols))

    def picked(zz, yy, k_from, v_from):
        k_out, v_out = None, None
        for b in range(bd):
            one = mask(zz, yy, b).astype(BF16)
            k_term, v_term = k_from(b) * one, v_from(b) * one
            k_out = k_term if k_out is None else k_out + k_term
            v_out = v_term if v_out is None else v_out + v_term
        return k_out, v_out

    def own_picked(zz, yy):
        return picked(zz, yy, lambda b: k_ref[b * BLK : (b + 1) * BLK, :], lambda b: v_ref[b * BLK : (b + 1) * BLK, :])

    @pl.when(mine_far)
    def _():
        for yy in range(g):
            a, b = own_picked(r, yy)
            fs[yy, 0] = a
            fs[yy, 1] = b
        each(1, g, lambda k: far_y_copy(lax.rem(y + k, g), y).start())
        ff[y] = fs[y]

    def own_rows(i):
        yy = y + 1 + i
        a, b = own_picked(z, yy)
        kvs[z, yy, 0] = a
        kvs[z, yy, 1] = b
        y_copy(z, yy, y).start()
    each(0, g - 1 - y, own_rows)

    loads[3].wait()
    width = x_ref.shape[1]
    w = width // tp
    eye = (iota((width, width), 0) == iota((width, width), 1)).astype(F32).astype(BF16)
    flipped = dot(eye, x_ref[...], 1, 1).astype(BF16)
    xs[...] = flipped.reshape(tp, w, tok)
    each_x1(0, lambda s: x1_copy(s, z).start())

    @pl.when(t == z)
    def _():
        xg[z] = xs[t]

    def clear(yy):
        kvt[z * g + yy] = jnp.zeros(kvt.shape[1:], BF16)
    each(y, g, clear)

    for i in (4, 5, 6):
        loads[i].wait()
    less = jnp.concatenate([-lse_ref[h : h + 1, :] for h in range(heads)], axis=1)
    owner = ids // bd
    for zz in range(r):
        need = jnp.zeros((g, wide), jnp.bool_)
        at = zz * g + iota((g, wide), 0)
        for s in range(sel):
            need = need | (owner[s : s + 1, :] == at)
        bias[zz] = jnp.where(need & (at < me), less, MASKED)
    low = iota((tok, cols), 1) < HD

    def stacked(ref):
        part = ref[...]
        zero = jnp.zeros_like(part)
        return jnp.concatenate([jnp.where(low, part, zero), jnp.where(low, zero, part)], axis=0)

    qs[...] = stacked(q_ref)
    cs[...] = stacked(c_ref)

    key_at = iota((tok, wide), 0)
    query_at = lax.rem(iota((tok, wide), 1), tok)
    own_block = key_at // BLK
    need = jnp.zeros((tok, wide), jnp.bool_)
    own_ids = jnp.where(owner == me, lax.rem(ids, bd), bd)
    for s in range(sel):
        need = need | (own_ids[s : s + 1, :] == own_block)
    need = need | ((own_block == query_at // BLK) & (key_at <= query_at))
    own = jnp.exp(dot(k_ref[...], qs[...], 1, 1) * scale + jnp.where(need, less, MASKED))
    vdo = dot(v_ref[...], cs[...], 1, 1)
    gvo[...] = dot(own.astype(BF16), cs[...], 1, 0)
    first = jnp.sum(own * vdo, axis=0, keepdims=True)

    def relay(i):
        zz = z - 1 - i

        @pl.when(~is_far(zz, z))
        def _():
            z_copy(zz, zz).wait_recv()

            for yy in range(g):
                a, b = picked(zz, yy, lambda b: kz[zz, 0, b * BLK : (b + 1) * BLK, :],
                              lambda b: kz[zz, 1, b * BLK : (b + 1) * BLK, :])
                kvs[zz, yy, 0] = a
                kvs[zz, yy, 1] = b
            each(1, g, lambda k: y_copy(zz, lax.rem(y + k, g), y).start())
            kvt[zz * g + y] = kvs[zz, y]
    once = jnp.minimum(z, 1)
    each(0, once, relay)

    @pl.when(mine_far)
    def _():
        arrived(ff.at[pl.ds(0, g - 1)], fyr.at[0])
        far_z_copy(z).start()
    each(once, z, relay)

    def send_back(c, zz):
        def one(k):
            yy = lax.rem(y + k, g)

            @pl.when((zz < z) | (yy < y))
            def _():
                back_copy(c, zz, yy, y).start()

        @pl.when(is_far_back(zz, z))
        def _():
            far_back_copy(c, zz).start()

        @pl.when(~is_far_back(zz, z))
        def _():
            each(1, g, one)
            back_r[c, zz, y] = back_s[c, zz, y]

    def pass_one(i, delta):
        zz = z - i

        @pl.when(is_far(zz, z))
        def _():
            far_z_copy(zz).wait_recv()

        @pl.when((zz < z) & ~is_far(zz, z))
        def _():
            arrived(kvt.at[pl.ds(zz * g, g - 1)], yr_sem.at[zz])

        @pl.when(zz == z)
        def _():
            counted(y, g - 1, lambda i: arrived(kvt.at[pl.ds(z * g, i)], yr_sem.at[z]))
        kp = kvt[pl.ds(zz * g, g), 0].reshape(chunk, cols)
        vp = kvt[pl.ds(zz * g, g), 1].reshape(chunk, cols)
        line = jnp.concatenate(
            [jnp.broadcast_to(bias[zz, a : a + 1, :], (BLK, wide)) for a in range(g)], axis=0)
        weights = jnp.exp(dot(kp, qs[...], 1, 1) * scale + line)
        vd = dot(vp, cs[...], 1, 1)
        wts[zz] = weights
        vds[zz] = vd
        back_s[1, zz] = dot(weights.astype(BF16), cs[...], 1, 0).astype(BF16).reshape(g, BLK, cols)
        send_back(1, zz)
        return delta + jnp.sum(weights * vd, axis=0, keepdims=True)
    middle = (z + 2) // 2
    delta = lax.fori_loop(0, middle, pass_one, first)

    counted(tp - jnp.where(t == z, 1, 0), tp, lambda i: arrived(xg.at[pl.ds(0, i)], x1r.at[0]))
    for i in range(1, tp):
        x2_copy(lax.rem(t + i, tp), t).start()
    xr[t] = xg[...]
    delta = lax.fori_loop(middle, z + 1, pass_one, delta)

    dso = (own * (vdo - delta)).astype(BF16)
    dqa[...] = dot(dso, k_ref[...], 0, 0)

    def key_grads(zz):
        back_s[0, zz] = (dot(dss[zz], qs[...], 1, 0) * scale).astype(BF16).reshape(g, BLK, cols)
        send_back(0, zz)

    def pass_two(zz):
        kp = kvt[pl.ds(zz * g, g), 0].reshape(chunk, cols)
        ds = (wts[zz] * (vds[zz] - delta)).astype(BF16)
        dss[zz] = ds
        dqa[...] += dot(ds, kp, 0, 0)

        @pl.when(is_far_back(zz, z))
        def _():
            key_grads(zz)
    each(0, z + 1, pass_two)

    dq = jnp.where(low, dqa[:tok], dqa[tok:]) * scale
    dq = dq.astype(BF16)
    gq_ref[...] = dq
    dqr[z] = dq
    for i in far_first(r):
        dq_copy(lax.rem(z + i, r), z).start()

    def other_key_grads(zz):
        @pl.when(~is_far_back(zz, z))
        def _():
            key_grads(zz)
    each(0, z + 1, other_key_grads)
    gko[...] = dot(dso, qs[...], 1, 0) * scale

    def relay_back(c, low_z, high_z, with_own):
        own_sum = gko if c == 0 else gvo

        def own_add(i):
            yy = y + 1 + i
            got = back_r[c, z, yy].astype(F32)
            for b in range(bd):
                own_sum[b * BLK : (b + 1) * BLK, :] += got * mask(z, yy, b)

        def one(i):
            zz = i if c == 0 else z - 1 - i

            @pl.when(~is_far_back(zz, z))
            def _():
                arrived(back_r.at[c, zz, pl.ds(0, g - 1)], br_sem.at[c, zz])
                sums = [None] * bd
                for yy in range(g):
                    got = back_r[c, zz, yy].astype(F32)
                    for b in range(bd):
                        term = got * mask(zz, yy, b)
                        sums[b] = term if sums[b] is None else sums[b] + term
                for b in range(bd):
                    rel_s[c, zz, b * BLK : (b + 1) * BLK, :] = sums[b].astype(BF16)
                rel_copy(c, zz, z).start()
        each(low_z, high_z, one)
        if with_own:
            counted(g - 1 - y, g - 1, lambda i: arrived(back_r.at[c, z, pl.ds(0, i)], br_sem.at[c, z]))
            each(0, g - 1 - y, own_add)

    def far_forward(c):
        @pl.when(mine_far_back)
        def _():
            far_back_copy(c, 0).wait_recv()
            for i in range(1, g):
                far_ret_copy(c, lax.rem(y + i, g), y).start()

    def far_add(c):
        own_sum = gko if c == 0 else gvo

        @pl.when(mine_far_back)
        def _():
            arrived(fr.at[c, pl.ds(0, g - 1)], frr.at[c])
            fr[c, y] = fb[c, y]
            sums = [own_sum[b * BLK : (b + 1) * BLK, :] for b in range(bd)]
            for yy in range(g):
                got = fr[c, yy].astype(F32)
                for b in range(bd):
                    sums[b] = sums[b] + got * mask(r, yy, b)
            for b in range(bd):
                own_sum[b * BLK : (b + 1) * BLK, :] = sums[b]

    relay_back(1, 0, z, True)
    far_forward(1)
    far_forward(0)
    half = z // 2
    relay_back(0, 0, half, False)

    arrived(xr.at[pl.ds(0, tp - 1)], x2r.at[0])
    arrived(dqr.at[pl.ds(0, r - 1)], dqr_sem.at[0])
    total = None
    for zz in range(r):
        part = dot(xr[:, zz].reshape(width, tok), dqr[zz], 1, 0)
        total = part if total is None else total + part
    for yy in range(g):
        gs[yy] = total[yy * w : (yy + 1) * w].astype(BF16)

        @pl.when(yy == y)
        def _():
            gw_ref[...] = total[yy * w : (yy + 1) * w]
    for i in far_first(g):
        gw_copy(lax.rem(y + i, g), y).start()

    relay_back(0, half, z, True)
    far_add(1)
    far_add(0)

    def settle(c):
        own_sum = gko if c == 0 else gvo

        def one(i):
            zz = z + 1 + i

            @pl.when(~is_far_back(z, zz))
            def _():
                rel_copy(c, 0, zz).wait_recv()
                own_sum[...] += rel_r[c, zz].astype(F32)
        each(0, r - 1 - z, one)
        (gk_ref if c == 0 else gv_ref)[...] = own_sum[...].astype(BF16)
    settle(1)
    settle(0)

    arrived(gr.at[pl.ds(0, g - 1)], gr_sem.at[0])
    for i in range(1, g):
        gw_ref[...] += gr[lax.rem(y + i, g)].astype(F32)

    in_far = jnp.where(z == r - 1, 1, 0) + jnp.where(z == r - 2, 1, 0)
    counted(r - 1 - z - jnp.where(mine_far, 1, 0), r - 1, lambda i: left(kz.at[pl.ds(0, i)], zs_sem.at[0]))
    counted(g - 1 - y, g - 1, lambda i: left(kvs.at[z, pl.ds(0, i)], ys_sem.at[z]))

    @pl.when(mine_far)
    def _():
        far_z_copy(z).wait_send()
        left(fs.at[pl.ds(0, g - 1)], fys.at[0])

    @pl.when(mine_far_back)
    def _():
        left(fb.at[0, pl.ds(0, g - 1)], frs.at[0])
        left(fb.at[1, pl.ds(0, g - 1)], frs.at[1])

    for c in range(2):
        counted(z - in_far, r - 1, lambda i: left(rel_s.at[c, pl.ds(0, i)], rs_sem.at[c]))
        counted(y, g - 1, lambda i: left(back_s.at[c, z, pl.ds(0, i)], bs_sem.at[c, z]))

    def sent_row(zz):
        @pl.when(~is_far(zz, z))
        def _():
            left(kvs.at[zz, pl.ds(0, g - 1)], ys_sem.at[zz])

        @pl.when(is_far_back(zz, z))
        def _():
            far_back_copy(0, zz).wait_send()
            far_back_copy(1, zz).wait_send()

        @pl.when(~is_far_back(zz, z))
        def _():
            left(back_s.at[0, zz, pl.ds(0, g - 1)], bs_sem.at[0, zz])
            left(back_s.at[1, zz, pl.ds(0, g - 1)], bs_sem.at[1, zz])
    each(0, z, sent_row)
    counted(tp - jnp.where(t == z, 1, 0), tp, lambda i: left(xs.at[pl.ds(0, i)], x1s.at[0]))
    left(xr.at[pl.ds(0, tp - 1)], x2s.at[0])
    left(dqr.at[pl.ds(0, r - 1)], dqs_sem.at[0])
    left(gs.at[pl.ds(0, g - 1)], gs_sem.at[0])


def write_out(*refs):
    sems = refs[8]
    copies = [pltpu.make_async_copy(refs[i], refs[4 + i], sems.at[i]) for i in range(4)]
    for copy in copies:
        copy.start()
    for copy in copies:
        copy.wait()


def body(g, r, tp, queries, keys, values, cotangent, log_sum, chosen, normed_input):
    tok, cols = queries.shape
    bd = tok // BLK
    wide = 2 * tok
    w = normed_input.shape[1] // tp
    vmem = pl.BlockSpec(memory_space=pltpu.VMEM)
    sem = pltpu.SemaphoreType.DMA
    hbm = pl.BlockSpec(memory_space=pltpu.HBM)
    picks = chosen.transpose(2, 0, 1)
    held = [pltpu.VMEM(a.shape, a.dtype) for a in (
        queries, jax.ShapeDtypeStruct((2, tok, cols), BF16), cotangent, log_sum, picks, normed_input)]
    made = pl.pallas_call(
        functools.partial(kernel, g, r, tp),
        out_shape=[
            jax.ShapeDtypeStruct((tok, cols), BF16),
            jax.ShapeDtypeStruct((tok, cols), BF16),
            jax.ShapeDtypeStruct((tok, cols), BF16),
            jax.ShapeDtypeStruct((w, cols), F32),
        ],
        in_specs=[hbm] * 7,
        out_specs=[vmem] * 4,
        scratch_shapes=held + [
            sem((7,)),
            pltpu.VMEM((wide, cols), BF16),
            pltpu.VMEM((wide, cols), BF16),
            pltpu.VMEM((r + 1, g, bd, cols), F32),
            pltpu.VMEM((r, g, wide), F32),
            pltpu.VMEM((r, 2, tok, cols), BF16),
            pltpu.VMEM((r, g, 2, BLK, cols), BF16),
            pltpu.VMEM((r * g, 2, BLK, cols), BF16),
            pltpu.VMEM((r, g * BLK, wide), F32),
            pltpu.VMEM((r, g * BLK, wide), F32),
            pltpu.VMEM((r, g * BLK, wide), BF16),
            pltpu.VMEM((2, r, g, BLK, cols), BF16),
            pltpu.VMEM((2, r, g, BLK, cols), BF16),
            pltpu.VMEM((2, r, tok, cols), BF16),
            pltpu.VMEM((2, r, tok, cols), BF16),
            pltpu.VMEM((tok, cols), F32),
            pltpu.VMEM((tok, cols), F32),
            pltpu.VMEM((wide, cols), F32),
            pltpu.VMEM((tp, w, tok), BF16),
            pltpu.VMEM((r, w, tok), BF16),
            pltpu.VMEM((tp, r, w, tok), BF16),
            pltpu.VMEM((r, tok, cols), BF16),
            pltpu.VMEM((g, w, cols), BF16),
            pltpu.VMEM((g, w, cols), BF16),
            pltpu.VMEM((g, 2, BLK, cols), BF16),
            pltpu.VMEM((g, 2, BLK, cols), BF16),
            pltpu.VMEM((2, g, BLK, cols), BF16),
            pltpu.VMEM((2, g, BLK, cols), BF16),
            sem((1,)), sem((r,)),
            sem((r,)), sem((r,)),
            sem((2, r)), sem((2, r)),
            sem((2,)), sem((2, r)),
            sem((1,)), sem((1,)),
            sem((1,)), sem((1,)),
            sem((1,)), sem((1,)),
            sem((1,)), sem((1,)),
            sem((1,)), sem((1,)),
            sem((1,)), sem((2,)),
            sem((2, 2)), sem((2,)),
            sem((2,)), sem((2,)),
        ],
        compiler_params=pltpu.CompilerParams(
            has_side_effects=True, collective_id=0, vmem_limit_bytes=67043328),
    )(queries, keys, values, cotangent, log_sum, picks, normed_input)
    return pl.pallas_call(
        write_out,
        out_shape=[jax.ShapeDtypeStruct(a.shape, a.dtype) for a in made],
        in_specs=[vmem] * 4,
        out_specs=[hbm] * 4,
        scratch_shapes=[sem((4,))],
    )(*made)


def solution(mesh):
    n, tp = mesh.shape["kv"], mesh.shape["tp"]
    g = n // tp
    in_specs = (
        P("kv", "tp"), P("kv", "tp"), P("kv", "tp"), P("kv", "tp"),
        P("tp", "kv"), P("tp", None, None), P("kv", "tp"),
    )
    out_specs = (P("kv", "tp"),) * 4
    return jax.shard_map(
        functools.partial(body, g, n // g, tp), mesh=mesh, in_specs=in_specs, out_specs=out_specs, check_vma=False
    )
```

```python
import functools

import jax
import jax.numpy as jnp
from jax import lax
from jax.experimental import pallas as pl
from jax.experimental.pallas import tpu as pltpu
from jax.sharding import PartitionSpec as P

HD = 64
BLK = 32
MASKED = -1e30
MESH = pl.DeviceIdType.MESH
F32 = jnp.float32
BF16 = jnp.bfloat16


def dot(a, b, ca, cb):
    return lax.dot_general(a, b, (((ca,), (cb,)), ((), ())), preferred_element_type=F32)


def iota(shape, dim):
    return lax.broadcasted_iota(jnp.int32, shape, dim)


def each(low, high, fn):
    def step(i, carry):
        fn(i)
        return carry
    lax.fori_loop(low, high, step, 0)


def far_first(n):
    return sorted(range(1, n), key=lambda i: -min(i, n - i))


def kernel(
    g, r, tp, q_in, k_in, v_in, c_in, lse_in, pick_in, x_in,
    gq_ref, gk_ref, gv_ref, gw_ref,
    q_ref, kv_ref, c_ref, lse_ref, pick_ref, x_ref, insem,
    qs, cs, hot, bias, kz, kvs, kvt, wts, vds, dss, back_s, back_r, rel_s, rel_r, gko, gvo, dqa,
    xs, xg, xr, dqr, gs, gr, fs, ff, fb, fr,
    zs_sem, zr_sem, ys_sem, yr_sem, bs_sem, br_sem, rs_sem, rr_sem,
    x1s, x1r, x2s, x2r, dqs_sem, dqr_sem, gs_sem, gr_sem,
    fys, fyr, fzs, fzr, fbs, fbr, frs, frr,
):
    k_ref, v_ref = kv_ref.at[0], kv_ref.at[1]
    tok, cols = q_ref.shape
    sel, heads, blocks = pick_ref.shape
    bd = tok // BLK
    wide = 2 * tok
    chunk = g * BLK
    scale = HD ** (-0.5)
    me, t = lax.axis_index("kv"), lax.axis_index("tp")
    z, y = me // g, lax.rem(me, g)

    def far_of(zz):
        return r - 1 - lax.rem(zz, 4) // 2

    def has_far(zz):
        return (lax.rem(zz, 2) == 0) & (zz < r - 2)

    def is_far(zz, to):
        return has_far(zz) & (far_of(zz) == to)

    def far_back(zz):
        return (zz == 2) | (zz == 4)

    def is_far_back(zz, to):
        return far_back(zz) & (far_of(zz) == to)
    far, mine_far, mine_far_back = far_of(z), has_far(z), far_back(z)

    loads = {}
    for i, (a, b) in enumerate((
        (pick_in, pick_ref), (k_in, k_ref), (v_in, v_ref), (x_in, x_ref),
        (q_in, q_ref), (c_in, c_ref), (lse_in, lse_ref),
    )):
        loads[i] = pltpu.make_async_copy(a, b, insem.at[i])
        loads[i].start()

    barrier = pltpu.get_barrier_semaphore()

    def greet(kv, tt):
        pl.semaphore_signal(barrier, inc=1, device_id=(kv, tt), device_id_type=MESH)

    for i in range(1, r):
        greet(lax.rem(z + i, r) * g + y, t)
    for i in range(1, g):
        greet(z * g + lax.rem(y + i, g), t)
    for i in range(1, tp):
        greet(me, lax.rem(t + i, tp))
    for i in range(r):
        zz = lax.rem(z + i, r)
        if i == 0:
            @pl.when(t != z)
            def _():
                greet(zz * g + y, z)
        else:
            greet(zz * g + y, z)

    def remote(src, dst, ssem, rsem, kv, tt):
        return pltpu.make_async_remote_copy(
            src_ref=src, dst_ref=dst, send_sem=ssem, recv_sem=rsem, device_id=(kv, tt), device_id_type=MESH)

    def z_copy(zz, slot):
        return remote(kv_ref, kz.at[slot], zs_sem.at[0], zr_sem.at[slot], zz * g + y, t)

    def y_copy(zz, yy, slot):
        return remote(kvs.at[zz, yy], kvt.at[zz * g + slot], ys_sem.at[zz], yr_sem.at[zz], z * g + yy, t)

    def far_y_copy(yy, slot):
        return remote(fs.at[yy], ff.at[slot], fys.at[0], fyr.at[0], z * g + yy, t)

    def far_z_copy(slot):
        return remote(ff, kvt.at[pl.ds(slot * g, g)], fzs.at[0], fzr.at[slot // 4], far * g + y, t)

    def far_back_copy(c, zz):
        return remote(back_s.at[c, zz], fb.at[c], fbs.at[c, zz // 4], fbr.at[c], zz * g + y, t)

    def far_ret_copy(c, yy, slot):
        return remote(fb.at[c, yy], fr.at[c, slot], frs.at[c], frr.at[c], z * g + yy, t)

    def back_copy(c, zz, yy, slot):
        return remote(back_s.at[c, zz, yy], back_r.at[c, zz, slot], bs_sem.at[c, zz], br_sem.at[c, zz], z * g + yy, t)

    def rel_copy(c, zz, slot):
        return remote(rel_s.at[c, zz], rel_r.at[c, slot], rs_sem.at[c], rr_sem.at[c, slot], zz * g + y, t)

    def x1_copy(s, slot):
        return remote(xs.at[s], xg.at[slot], x1s.at[0], x1r.at[0], t * g + y, s)

    def x2_copy(tt, slot):
        return remote(xg, xr.at[slot], x2s.at[0], x2r.at[0], me, tt)

    def dq_copy(zz, slot):
        return remote(dqr.at[z], dqr.at[slot], dqs_sem.at[0], dqr_sem.at[0], zz * g + y, t)

    def gw_copy(yy, slot):
        return remote(gs.at[yy], gr.at[slot], gs_sem.at[0], gr_sem.at[0], z * g + yy, t)

    other = z * g + lax.rem(y + 1, g)

    def arrived(ref, sem):
        remote(ref, ref, sem, sem, other, t).wait_recv()

    def left(ref, sem):
        remote(ref, ref, sem, sem, other, t).wait_send()

    def counted(count, most, fn):
        for i in range(1, most + 1):
            @pl.when(count == i)
            def _():
                fn(i)

    def each_x1(low, fn):
        def step(s):
            @pl.when((t != z) | (s != t))
            def _():
                fn(s)
        each(low, tp, step)

    loads[0].wait()
    block_of = iota((blocks, heads * g * bd), 0)
    col_of = iota((blocks, heads * g * bd), 1)
    at_row = lax.rem(col_of, g * bd) == block_of - z * (g * bd)
    at_far = lax.rem(col_of, g * bd) == block_of - far * (g * bd)
    at_tok = me * bd + lax.rem(iota((blocks, heads * tok), 1), tok) // BLK == iota((blocks, heads * tok), 0)
    tok_head = iota((blocks, heads * tok), 1) // tok
    row_ids, far_ids, ids = None, None, None
    for h in range(heads):
        mine = pick_ref[:, h, :].astype(F32).astype(BF16)
        pick_row = (at_row & (col_of // (g * bd) == h)).astype(F32).astype(BF16)
        pick_far = (at_far & (col_of // (g * bd) == h)).astype(F32).astype(BF16)
        pick_tok = (at_tok & (tok_head == h)).astype(F32).astype(BF16)
        a, b, f = dot(mine, pick_row, 1, 0), dot(mine, pick_tok, 1, 0), dot(mine, pick_far, 1, 0)
        far_ids = f if far_ids is None else far_ids + f
        row_ids = a if row_ids is None else row_ids + a
        ids = b if ids is None else ids + b
    row_ids = (row_ids + 0.5).astype(jnp.int32)
    far_ids = (far_ids + 0.5).astype(jnp.int32)
    ids = (ids + 0.5).astype(jnp.int32)
    ids = jnp.where(ids < me * bd + lax.rem(iota(ids.shape, 1), tok) // BLK, ids, blocks)
    target_at = iota((r * bd, heads * g * bd), 0)
    target = (target_at // bd * g + y) * bd + lax.rem(target_at, bd)
    hit = jnp.zeros(target.shape, F32)
    own_target = me * bd + iota((2 * bd, heads * g * bd), 0)
    far_hit = jnp.zeros(own_target.shape, F32)
    for s in range(sel):
        hit = jnp.where(row_ids[s : s + 1, :] == target, 1.0, hit)
        far_hit = jnp.where(far_ids[s : s + 1, :] == own_target, 1.0, far_hit)
    out_at, out_from = iota((heads * g * bd, g * cols), 1), iota((heads * g * bd, g * cols), 0)
    fan = (lax.rem(out_from, g * bd) // bd == out_at // cols) & (
        lax.rem(out_at, cols) // HD == out_from // (g * bd))
    fan = fan.astype(F32).astype(BF16)
    far_taken = jnp.where(dot(far_hit.astype(BF16), fan, 1, 0) > 0.5, 1.0, 0.0)
    taken = dot(hit.astype(BF16), fan, 1, 0)
    taken = jnp.where(taken > 0.5, 1.0, 0.0).reshape(r, bd, g * cols)
    for yy in range(g):
        hot[:r, yy] = taken[:, :, yy * cols : (yy + 1) * cols]
        hot[r, yy] = far_taken[:bd, yy * cols : (yy + 1) * cols]

    loads[1].wait()
    loads[2].wait()
    pl.semaphore_wait(barrier, (r - 1) + (g - 1) + (tp - 1) + r - jnp.where(t == z, 1, 0))

    def span(i):
        zz = z + 1 + i

        @pl.when(~is_far(z, zz))
        def _():
            z_copy(zz, z).start()
    each(0, r - 1 - z, span)

    def mask(zz, yy, b):
        return jnp.broadcast_to(hot[zz, yy, pl.ds(b, 1), :], (BLK, cols))

    def picked(zz, yy, k_from, v_from):
        k_out, v_out = None, None
        for b in range(bd):
            one = mask(zz, yy, b).astype(BF16)
            k_term, v_term = k_from(b) * one, v_from(b) * one
            k_out = k_term if k_out is None else k_out + k_term
            v_out = v_term if v_out is None else v_out + v_term
        return k_out, v_out

    def own_picked(zz, yy):
        return picked(zz, yy, lambda b: k_ref[b * BLK : (b + 1) * BLK, :], lambda b: v_ref[b * BLK : (b + 1) * BLK, :])

    @pl.when(mine_far)
    def _():
        for yy in range(g):
            a, b = own_picked(r, yy)
            fs[yy, 0] = a
            fs[yy, 1] = b
        for k in far_first(g):
            far_y_copy(lax.rem(y + k, g), y).start()
        ff[y] = fs[y]

    def own_rows(i):
        yy = y + 1 + i
        a, b = own_picked(z, yy)
        kvs[z, yy, 0] = a
        kvs[z, yy, 1] = b
        y_copy(z, yy, y).start()
    each(0, g - 1 - y, own_rows)

    def clear(yy):
        kvt[z * g + yy] = jnp.zeros(kvt.shape[1:], BF16)
    each(y, g, clear)

    for i in (4, 5, 6):
        loads[i].wait()
    less = jnp.concatenate([-lse_ref[h : h + 1, :] for h in range(heads)], axis=1)
    owner = ids // bd
    for zz in range(r):
        need = jnp.zeros((g, wide), jnp.bool_)
        at = zz * g + iota((g, wide), 0)
        for s in range(sel):
            need = need | (owner[s : s + 1, :] == at)
        bias[zz] = jnp.where(need & (at < me), less, MASKED)
    low = iota((tok, cols), 1) < HD

    def stacked(ref):
        part = ref[...]
        zero = jnp.zeros_like(part)
        return jnp.concatenate([jnp.where(low, part, zero), jnp.where(low, zero, part)], axis=0)

    qs[...] = stacked(q_ref)
    cs[...] = stacked(c_ref)

    key_at = iota((tok, wide), 0)
    query_at = lax.rem(iota((tok, wide), 1), tok)
    own_block = key_at // BLK
    need = jnp.zeros((tok, wide), jnp.bool_)
    own_ids = jnp.where(owner == me, lax.rem(ids, bd), bd)
    for s in range(sel):
        need = need | (own_ids[s : s + 1, :] == own_block)
    need = need | ((own_block == query_at // BLK) & (key_at <= query_at))
    own = jnp.exp(dot(k_ref[...], qs[...], 1, 1) * scale + jnp.where(need, less, MASKED))
    vdo = dot(v_ref[...], cs[...], 1, 1)
    gvo[...] = dot(own.astype(BF16), cs[...], 1, 0)
    first = jnp.sum(own * vdo, axis=0, keepdims=True)

    def relay(i):
        zz = z - 1 - i

        @pl.when(~is_far(zz, z))
        def _():
            z_copy(zz, zz).wait_recv()

            for yy in range(g):
                a, b = picked(zz, yy, lambda b: kz[zz, 0, b * BLK : (b + 1) * BLK, :],
                              lambda b: kz[zz, 1, b * BLK : (b + 1) * BLK, :])
                kvs[zz, yy, 0] = a
                kvs[zz, yy, 1] = b
            for k in far_first(g):
                y_copy(zz, lax.rem(y + k, g), y).start()
            kvt[zz * g + y] = kvs[zz, y]
    once = jnp.minimum(z, 1)
    each(0, once, relay)

    @pl.when(mine_far)
    def _():
        arrived(ff.at[pl.ds(0, g - 1)], fyr.at[0])
        far_z_copy(z).start()
    each(once, z, relay)

    loads[3].wait()
    width = x_ref.shape[1]
    w = width // tp
    eye = (iota((width, width), 0) == iota((width, width), 1)).astype(F32).astype(BF16)
    flipped = dot(eye, x_ref[...], 1, 1).astype(BF16)
    xs[...] = flipped.reshape(tp, w, tok)
    each_x1(0, lambda s: x1_copy(s, z).start())

    @pl.when(t == z)
    def _():
        xg[z] = xs[t]

    def send_back(c, zz):
        def one(k):
            yy = lax.rem(y + k, g)

            @pl.when((zz < z) | (yy < y))
            def _():
                back_copy(c, zz, yy, y).start()

        @pl.when(is_far_back(zz, z))
        def _():
            far_back_copy(c, zz).start()

        @pl.when(~is_far_back(zz, z))
        def _():
            for k in far_first(g):
                one(k)
            back_r[c, zz, y] = back_s[c, zz, y]

    def pass_one(i, delta):
        zz = z - i

        @pl.when(is_far(zz, z))
        def _():
            far_z_copy(zz).wait_recv()

        @pl.when((zz < z) & ~is_far(zz, z))
        def _():
            arrived(kvt.at[pl.ds(zz * g, g - 1)], yr_sem.at[zz])

        @pl.when(zz == z)
        def _():
            counted(y, g - 1, lambda i: arrived(kvt.at[pl.ds(z * g, i)], yr_sem.at[z]))
        kp = kvt[pl.ds(zz * g, g), 0].reshape(chunk, cols)
        vp = kvt[pl.ds(zz * g, g), 1].reshape(chunk, cols)
        line = jnp.concatenate(
            [jnp.broadcast_to(bias[zz, a : a + 1, :], (BLK, wide)) for a in range(g)], axis=0)
        weights = jnp.exp(dot(kp, qs[...], 1, 1) * scale + line)
        vd = dot(vp, cs[...], 1, 1)
        wts[zz] = weights
        vds[zz] = vd
        back_s[1, zz] = dot(weights.astype(BF16), cs[...], 1, 0).astype(BF16).reshape(g, BLK, cols)
        send_back(1, zz)
        return delta + jnp.sum(weights * vd, axis=0, keepdims=True)
    delta = lax.fori_loop(0, z + 1, pass_one, first)

    dso = (own * (vdo - delta)).astype(BF16)
    dqa[...] = dot(dso, k_ref[...], 0, 0)

    def key_grads(zz):
        back_s[0, zz] = (dot(dss[zz], qs[...], 1, 0) * scale).astype(BF16).reshape(g, BLK, cols)
        send_back(0, zz)

    def pass_two(zz):
        kp = kvt[pl.ds(zz * g, g), 0].reshape(chunk, cols)
        ds = (wts[zz] * (vds[zz] - delta)).astype(BF16)
        dss[zz] = ds
        dqa[...] += dot(ds, kp, 0, 0)

        @pl.when(is_far_back(zz, z))
        def _():
            key_grads(zz)
    each(0, z + 1, pass_two)

    dq = jnp.where(low, dqa[:tok], dqa[tok:]) * scale
    dq = dq.astype(BF16)
    gq_ref[...] = dq
    dqr[z] = dq
    for i in far_first(r):
        dq_copy(lax.rem(z + i, r), z).start()

    def other_key_grads(zz):
        @pl.when(~is_far_back(zz, z))
        def _():
            key_grads(zz)
    each(0, z + 1, other_key_grads)

    counted(tp - jnp.where(t == z, 1, 0), tp, lambda i: arrived(xg.at[pl.ds(0, i)], x1r.at[0]))
    for i in range(1, tp):
        x2_copy(lax.rem(t + i, tp), t).start()
    xr[t] = xg[...]
    gko[...] = dot(dso, qs[...], 1, 0) * scale

    def relay_back(c, low_z, high_z, with_own):
        own_sum = gko if c == 0 else gvo

        def own_add(i):
            yy = y + 1 + i
            got = back_r[c, z, yy].astype(F32)
            for b in range(bd):
                own_sum[b * BLK : (b + 1) * BLK, :] += got * mask(z, yy, b)

        def one(i):
            zz = i if c == 0 else z - 1 - i

            @pl.when(~is_far_back(zz, z))
            def _():
                arrived(back_r.at[c, zz, pl.ds(0, g - 1)], br_sem.at[c, zz])
                sums = [None] * bd
                for yy in range(g):
                    got = back_r[c, zz, yy].astype(F32)
                    for b in range(bd):
                        term = got * mask(zz, yy, b)
                        sums[b] = term if sums[b] is None else sums[b] + term
                for b in range(bd):
                    rel_s[c, zz, b * BLK : (b + 1) * BLK, :] = sums[b].astype(BF16)
                rel_copy(c, zz, z).start()
        each(low_z, high_z, one)
        if with_own:
            counted(g - 1 - y, g - 1, lambda i: arrived(back_r.at[c, z, pl.ds(0, i)], br_sem.at[c, z]))
            each(0, g - 1 - y, own_add)

    def far_forward(c):
        @pl.when(mine_far_back)
        def _():
            far_back_copy(c, 0).wait_recv()
            for i in far_first(g):
                far_ret_copy(c, lax.rem(y + i, g), y).start()

    def far_add(c):
        own_sum = gko if c == 0 else gvo

        @pl.when(mine_far_back)
        def _():
            arrived(fr.at[c, pl.ds(0, g - 1)], frr.at[c])
            fr[c, y] = fb[c, y]
            sums = [own_sum[b * BLK : (b + 1) * BLK, :] for b in range(bd)]
            for yy in range(g):
                got = fr[c, yy].astype(F32)
                for b in range(bd):
                    sums[b] = sums[b] + got * mask(r, yy, b)
            for b in range(bd):
                own_sum[b * BLK : (b + 1) * BLK, :] = sums[b]

    relay_back(1, 0, z, True)
    far_forward(1)
    far_forward(0)
    half = z // 2
    relay_back(0, 0, half, False)

    arrived(xr.at[pl.ds(0, tp - 1)], x2r.at[0])
    arrived(dqr.at[pl.ds(0, r - 1)], dqr_sem.at[0])
    total = None
    for zz in range(r):
        part = dot(xr[:, zz].reshape(width, tok), dqr[zz], 1, 0)
        total = part if total is None else total + part
    for yy in range(g):
        gs[yy] = total[yy * w : (yy + 1) * w].astype(BF16)

        @pl.when(yy == y)
        def _():
            gw_ref[...] = total[yy * w : (yy + 1) * w]
    for i in far_first(g):
        gw_copy(lax.rem(y + i, g), y).start()

    relay_back(0, half, z, True)
    far_add(1)
    far_add(0)

    def settle(c):
        own_sum = gko if c == 0 else gvo

        def one(i):
            zz = z + 1 + i

            @pl.when(~is_far_back(z, zz))
            def _():
                rel_copy(c, 0, zz).wait_recv()
                own_sum[...] += rel_r[c, zz].astype(F32)
        each(0, r - 1 - z, one)
        (gk_ref if c == 0 else gv_ref)[...] = own_sum[...].astype(BF16)
    settle(1)
    settle(0)

    arrived(gr.at[pl.ds(0, g - 1)], gr_sem.at[0])
    for i in range(1, g):
        gw_ref[...] += gr[lax.rem(y + i, g)].astype(F32)

    in_far = jnp.where(z == r - 1, 1, 0) + jnp.where(z == r - 2, 1, 0)
    counted(r - 1 - z - jnp.where(mine_far, 1, 0), r - 1, lambda i: left(kz.at[pl.ds(0, i)], zs_sem.at[0]))
    counted(g - 1 - y, g - 1, lambda i: left(kvs.at[z, pl.ds(0, i)], ys_sem.at[z]))

    @pl.when(mine_far)
    def _():
        far_z_copy(z).wait_send()
        left(fs.at[pl.ds(0, g - 1)], fys.at[0])

    @pl.when(mine_far_back)
    def _():
        left(fb.at[0, pl.ds(0, g - 1)], frs.at[0])
        left(fb.at[1, pl.ds(0, g - 1)], frs.at[1])

    for c in range(2):
        counted(z - in_far, r - 1, lambda i: left(rel_s.at[c, pl.ds(0, i)], rs_sem.at[c]))
        counted(y, g - 1, lambda i: left(back_s.at[c, z, pl.ds(0, i)], bs_sem.at[c, z]))

    def sent_row(zz):
        @pl.when(~is_far(zz, z))
        def _():
            left(kvs.at[zz, pl.ds(0, g - 1)], ys_sem.at[zz])

        @pl.when(is_far_back(zz, z))
        def _():
            far_back_copy(0, zz).wait_send()
            far_back_copy(1, zz).wait_send()

        @pl.when(~is_far_back(zz, z))
        def _():
            left(back_s.at[0, zz, pl.ds(0, g - 1)], bs_sem.at[0, zz])
            left(back_s.at[1, zz, pl.ds(0, g - 1)], bs_sem.at[1, zz])
    each(0, z, sent_row)
    counted(tp - jnp.where(t == z, 1, 0), tp, lambda i: left(xs.at[pl.ds(0, i)], x1s.at[0]))
    left(xr.at[pl.ds(0, tp - 1)], x2s.at[0])
    left(dqr.at[pl.ds(0, r - 1)], dqs_sem.at[0])
    left(gs.at[pl.ds(0, g - 1)], gs_sem.at[0])


def write_out(*refs):
    sems = refs[8]
    copies = [pltpu.make_async_copy(refs[i], refs[4 + i], sems.at[i]) for i in range(4)]
    for copy in copies:
        copy.start()
    for copy in copies:
        copy.wait()


def body(g, r, tp, queries, keys, values, cotangent, log_sum, chosen, normed_input):
    tok, cols = queries.shape
    bd = tok // BLK
    wide = 2 * tok
    w = normed_input.shape[1] // tp
    vmem = pl.BlockSpec(memory_space=pltpu.VMEM)
    sem = pltpu.SemaphoreType.DMA
    hbm = pl.BlockSpec(memory_space=pltpu.HBM)
    picks = chosen.transpose(2, 0, 1)
    held = [pltpu.VMEM(a.shape, a.dtype) for a in (
        queries, jax.ShapeDtypeStruct((2, tok, cols), BF16), cotangent, log_sum, picks, normed_input)]
    made = pl.pallas_call(
        functools.partial(kernel, g, r, tp),
        out_shape=[
            jax.ShapeDtypeStruct((tok, cols), BF16),
            jax.ShapeDtypeStruct((tok, cols), BF16),
            jax.ShapeDtypeStruct((tok, cols), BF16),
            jax.ShapeDtypeStruct((w, cols), F32),
        ],
        in_specs=[hbm] * 7,
        out_specs=[vmem] * 4,
        scratch_shapes=held + [
            sem((7,)),
            pltpu.VMEM((wide, cols), BF16),
            pltpu.VMEM((wide, cols), BF16),
            pltpu.VMEM((r + 1, g, bd, cols), F32),
            pltpu.VMEM((r, g, wide), F32),
            pltpu.VMEM((r, 2, tok, cols), BF16),
            pltpu.VMEM((r, g, 2, BLK, cols), BF16),
            pltpu.VMEM((r * g, 2, BLK, cols), BF16),
            pltpu.VMEM((r, g * BLK, wide), F32),
            pltpu.VMEM((r, g * BLK, wide), F32),
            pltpu.VMEM((r, g * BLK, wide), BF16),
            pltpu.VMEM((2, r, g, BLK, cols), BF16),
            pltpu.VMEM((2, r, g, BLK, cols), BF16),
            pltpu.VMEM((2, r, tok, cols), BF16),
            pltpu.VMEM((2, r, tok, cols), BF16),
            pltpu.VMEM((tok, cols), F32),
            pltpu.VMEM((tok, cols), F32),
            pltpu.VMEM((wide, cols), F32),
            pltpu.VMEM((tp, w, tok), BF16),
            pltpu.VMEM((r, w, tok), BF16),
            pltpu.VMEM((tp, r, w, tok), BF16),
            pltpu.VMEM((r, tok, cols), BF16),
            pltpu.VMEM((g, w, cols), BF16),
            pltpu.VMEM((g, w, cols), BF16),
            pltpu.VMEM((g, 2, BLK, cols), BF16),
            pltpu.VMEM((g, 2, BLK, cols), BF16),
            pltpu.VMEM((2, g, BLK, cols), BF16),
            pltpu.VMEM((2, g, BLK, cols), BF16),
            sem((1,)), sem((r,)),
            sem((r,)), sem((r,)),
            sem((2, r)), sem((2, r)),
            sem((2,)), sem((2, r)),
            sem((1,)), sem((1,)),
            sem((1,)), sem((1,)),
            sem((1,)), sem((1,)),
            sem((1,)), sem((1,)),
            sem((1,)), sem((1,)),
            sem((1,)), sem((2,)),
            sem((2, 2)), sem((2,)),
            sem((2,)), sem((2,)),
        ],
        compiler_params=pltpu.CompilerParams(
            has_side_effects=True, collective_id=0, vmem_limit_bytes=67043328),
    )(queries, keys, values, cotangent, log_sum, picks, normed_input)
    return pl.pallas_call(
        write_out,
        out_shape=[jax.ShapeDtypeStruct(a.shape, a.dtype) for a in made],
        in_specs=[vmem] * 4,
        out_specs=[hbm] * 4,
        scratch_shapes=[sem((4,))],
    )(*made)


def solution(mesh):
    n, tp = mesh.shape["kv"], mesh.shape["tp"]
    g = n // tp
    in_specs = (
        P("kv", "tp"), P("kv", "tp"), P("kv", "tp"), P("kv", "tp"),
        P("tp", "kv"), P("tp", None, None), P("kv", "tp"),
    )
    out_specs = (P("kv", "tp"),) * 4
    return jax.shard_map(
        functools.partial(body, g, n // g, tp), mesh=mesh, in_specs=in_specs, out_specs=out_specs, check_vma=False
    )
```

```python
import functools

import jax
import jax.numpy as jnp
from jax import lax
from jax.experimental import pallas as pl
from jax.experimental.pallas import tpu as pltpu
from jax.sharding import PartitionSpec as P

HD = 64
BLK = 32
MASKED = -1e30
MESH = pl.DeviceIdType.MESH
F32 = jnp.float32
BF16 = jnp.bfloat16


def dot(a, b, ca, cb):
    return lax.dot_general(a, b, (((ca,), (cb,)), ((), ())), preferred_element_type=F32)


def iota(shape, dim):
    return lax.broadcasted_iota(jnp.int32, shape, dim)


def each(low, high, fn):
    def step(i, carry):
        fn(i)
        return carry
    lax.fori_loop(low, high, step, 0)


def far_first(n):
    return sorted(range(1, n), key=lambda i: -min(i, n - i))


def kernel(
    g, r, tp, q_in, k_in, v_in, c_in, lse_in, pick_in, x_in,
    gq_ref, gk_ref, gv_ref, gw_ref,
    q_ref, kv_ref, c_ref, lse_ref, pick_ref, x_ref, insem,
    qs, cs, hot, bias, kz, kvs, kvt, wts, vds, dss, back_s, back_r, rel_s, rel_r, gko, gvo, dqa,
    xs, xg, xr, dqr, gs, gr, fs, ff, fb, fr,
    zs_sem, zr_sem, ys_sem, yr_sem, bs_sem, br_sem, rs_sem, rr_sem,
    x1s, x1r, x2s, x2r, dqs_sem, dqr_sem, gs_sem, gr_sem,
    fys, fyr, fzs, fzr, fbs, fbr, frs, frr,
):
    k_ref, v_ref = kv_ref.at[0], kv_ref.at[1]
    tok, cols = q_ref.shape
    sel, heads, blocks = pick_ref.shape
    bd = tok // BLK
    wide = 2 * tok
    chunk = g * BLK
    scale = HD ** (-0.5)
    me, t = lax.axis_index("kv"), lax.axis_index("tp")
    z, y = me // g, lax.rem(me, g)

    def far_of(zz):
        return r - 1 - lax.rem(zz, 4) // 2

    def has_far(zz):
        return (lax.rem(zz, 2) == 0) & (zz < r - 2)

    def is_far(zz, to):
        return has_far(zz) & (far_of(zz) == to)

    def far_back(zz):
        return (zz == 2) | (zz == 4)

    def is_far_back(zz, to):
        return far_back(zz) & (far_of(zz) == to)
    far, mine_far, mine_far_back = far_of(z), has_far(z), far_back(z)

    loads = {}
    for i, (a, b) in enumerate((
        (pick_in, pick_ref), (k_in, k_ref), (v_in, v_ref), (x_in, x_ref),
        (q_in, q_ref), (c_in, c_ref), (lse_in, lse_ref),
    )):
        loads[i] = pltpu.make_async_copy(a, b, insem.at[i])
        loads[i].start()

    barrier = pltpu.get_barrier_semaphore()

    def greet(kv, tt):
        pl.semaphore_signal(barrier, inc=1, device_id=(kv, tt), device_id_type=MESH)

    for i in range(1, r):
        greet(lax.rem(z + i, r) * g + y, t)
    for i in range(1, g):
        greet(z * g + lax.rem(y + i, g), t)
    for i in range(1, tp):
        greet(me, lax.rem(t + i, tp))
    for i in range(r):
        zz = lax.rem(z + i, r)
        if i == 0:
            @pl.when(t != z)
            def _():
                greet(zz * g + y, z)
        else:
            greet(zz * g + y, z)

    def remote(src, dst, ssem, rsem, kv, tt):
        return pltpu.make_async_remote_copy(
            src_ref=src, dst_ref=dst, send_sem=ssem, recv_sem=rsem, device_id=(kv, tt), device_id_type=MESH)

    def z_copy(zz, slot):
        return remote(kv_ref, kz.at[slot], zs_sem.at[0], zr_sem.at[slot], zz * g + y, t)

    def y_copy(zz, yy, slot):
        return remote(kvs.at[zz, yy], kvt.at[zz * g + slot], ys_sem.at[0], yr_sem.at[zz], z * g + yy, t)

    def far_y_copy(yy, slot):
        return remote(fs.at[yy], ff.at[slot], fys.at[0], fyr.at[0], z * g + yy, t)

    def far_z_copy(slot):
        return remote(ff, kvt.at[pl.ds(slot * g, g)], fzs.at[0], fzr.at[slot // 4], far * g + y, t)

    def far_back_copy(c, zz):
        return remote(back_s.at[c, zz], fb.at[c], fbs.at[c, zz // 4], fbr.at[c], zz * g + y, t)

    def far_ret_copy(c, yy, slot):
        return remote(fb.at[c, yy], fr.at[c, slot], frs.at[c], frr.at[c], z * g + yy, t)

    def back_copy(c, zz, yy, slot):
        return remote(back_s.at[c, zz, yy], back_r.at[c, zz, slot], bs_sem.at[c], br_sem.at[c, zz], z * g + yy, t)

    def rel_copy(c, zz, slot):
        return remote(rel_s.at[c, zz], rel_r.at[c, slot], rs_sem.at[c], rr_sem.at[c, slot], zz * g + y, t)

    def x1_copy(s, slot):
        return remote(xs.at[s], xg.at[slot], x1s.at[0], x1r.at[0], t * g + y, s)

    def x2_copy(tt, slot):
        return remote(xg, xr.at[slot], x2s.at[0], x2r.at[0], me, tt)

    def dq_copy(zz, slot):
        return remote(dqr.at[z], dqr.at[slot], dqs_sem.at[0], dqr_sem.at[0], zz * g + y, t)

    def gw_copy(yy, slot):
        return remote(gs.at[yy], gr.at[slot], gs_sem.at[0], gr_sem.at[0], z * g + yy, t)

    other = z * g + lax.rem(y + 1, g)

    def arrived(ref, sem):
        remote(ref, ref, sem, sem, other, t).wait_recv()

    def left(ref, sem):
        remote(ref, ref, sem, sem, other, t).wait_send()

    def counted(count, most, fn):
        for i in range(1, most + 1):
            @pl.when(count == i)
            def _():
                fn(i)

    def each_x1(low, fn):
        def step(s):
            @pl.when((t != z) | (s != t))
            def _():
                fn(s)
        each(low, tp, step)

    loads[0].wait()
    block_of = iota((blocks, heads * g * bd), 0)
    col_of = iota((blocks, heads * g * bd), 1)
    at_row = lax.rem(col_of, g * bd) == block_of - z * (g * bd)
    at_far = lax.rem(col_of, g * bd) == block_of - far * (g * bd)
    at_tok = me * bd + lax.rem(iota((blocks, heads * tok), 1), tok) // BLK == iota((blocks, heads * tok), 0)
    tok_head = iota((blocks, heads * tok), 1) // tok
    row_ids, far_ids, ids = None, None, None
    for h in range(heads):
        mine = pick_ref[:, h, :].astype(F32).astype(BF16)
        pick_row = (at_row & (col_of // (g * bd) == h)).astype(F32).astype(BF16)
        pick_far = (at_far & (col_of // (g * bd) == h)).astype(F32).astype(BF16)
        pick_tok = (at_tok & (tok_head == h)).astype(F32).astype(BF16)
        a, b, f = dot(mine, pick_row, 1, 0), dot(mine, pick_tok, 1, 0), dot(mine, pick_far, 1, 0)
        far_ids = f if far_ids is None else far_ids + f
        row_ids = a if row_ids is None else row_ids + a
        ids = b if ids is None else ids + b
    row_ids = (row_ids + 0.5).astype(jnp.int32)
    far_ids = (far_ids + 0.5).astype(jnp.int32)
    ids = (ids + 0.5).astype(jnp.int32)
    ids = jnp.where(ids < me * bd + lax.rem(iota(ids.shape, 1), tok) // BLK, ids, blocks)
    target_at = iota((r * bd, heads * g * bd), 0)
    target = (target_at // bd * g + y) * bd + lax.rem(target_at, bd)
    hit = jnp.zeros(target.shape, F32)
    own_target = me * bd + iota((2 * bd, heads * g * bd), 0)
    far_hit = jnp.zeros(own_target.shape, F32)
    for s in range(sel):
        hit = jnp.where(row_ids[s : s + 1, :] == target, 1.0, hit)
        far_hit = jnp.where(far_ids[s : s + 1, :] == own_target, 1.0, far_hit)
    out_at, out_from = iota((heads * g * bd, g * cols), 1), iota((heads * g * bd, g * cols), 0)
    fan = (lax.rem(out_from, g * bd) // bd == out_at // cols) & (
        lax.rem(out_at, cols) // HD == out_from // (g * bd))
    fan = fan.astype(F32).astype(BF16)
    far_taken = jnp.where(dot(far_hit.astype(BF16), fan, 1, 0) > 0.5, 1.0, 0.0)
    taken = dot(hit.astype(BF16), fan, 1, 0)
    taken = jnp.where(taken > 0.5, 1.0, 0.0).reshape(r, bd, g * cols)
    for yy in range(g):
        hot[:r, yy] = taken[:, :, yy * cols : (yy + 1) * cols]
        hot[r, yy] = far_taken[:bd, yy * cols : (yy + 1) * cols]

    loads[1].wait()
    loads[2].wait()
    pl.semaphore_wait(barrier, (r - 1) + (g - 1) + (tp - 1) + r - jnp.where(t == z, 1, 0))

    def span(i):
        zz = z + 1 + i

        @pl.when(~is_far(z, zz))
        def _():
            z_copy(zz, z).start()
    each(0, r - 1 - z, span)

    def mask(zz, yy, b):
        return jnp.broadcast_to(hot[zz, yy, pl.ds(b, 1), :], (BLK, cols))

    def picked(zz, yy, k_from, v_from):
        k_out, v_out = None, None
        for b in range(bd):
            one = mask(zz, yy, b).astype(BF16)
            k_term, v_term = k_from(b) * one, v_from(b) * one
            k_out = k_term if k_out is None else k_out + k_term
            v_out = v_term if v_out is None else v_out + v_term
        return k_out, v_out

    def own_picked(zz, yy):
        return picked(zz, yy, lambda b: k_ref[b * BLK : (b + 1) * BLK, :], lambda b: v_ref[b * BLK : (b + 1) * BLK, :])

    @pl.when(mine_far)
    def _():
        for yy in range(g):
            a, b = own_picked(r, yy)
            fs[yy, 0] = a
            fs[yy, 1] = b
        for k in far_first(g):
            far_y_copy(lax.rem(y + k, g), y).start()
        ff[y] = fs[y]

    def own_rows(i):
        yy = y + 1 + i
        a, b = own_picked(z, yy)
        kvs[z, yy, 0] = a
        kvs[z, yy, 1] = b
        y_copy(z, yy, y).start()
    each(0, g - 1 - y, own_rows)

    def clear(yy):
        kvt[z * g + yy] = jnp.zeros(kvt.shape[1:], BF16)
    each(y, g, clear)

    for i in (4, 5, 6):
        loads[i].wait()
    less = jnp.concatenate([-lse_ref[h : h + 1, :] for h in range(heads)], axis=1)
    owner = ids // bd
    for zz in range(r):
        need = jnp.zeros((g, wide), jnp.bool_)
        at = zz * g + iota((g, wide), 0)
        for s in range(sel):
            need = need | (owner[s : s + 1, :] == at)
        bias[zz] = jnp.where(need & (at < me), less, MASKED)
    low = iota((tok, cols), 1) < HD

    def stacked(ref):
        part = ref[...]
        zero = jnp.zeros_like(part)
        return jnp.concatenate([jnp.where(low, part, zero), jnp.where(low, zero, part)], axis=0)

    qs[...] = stacked(q_ref)
    cs[...] = stacked(c_ref)

    key_at = iota((tok, wide), 0)
    query_at = lax.rem(iota((tok, wide), 1), tok)
    own_block = key_at // BLK
    need = jnp.zeros((tok, wide), jnp.bool_)
    own_ids = jnp.where(owner == me, lax.rem(ids, bd), bd)
    for s in range(sel):
        need = need | (own_ids[s : s + 1, :] == own_block)
    need = need | ((own_block == query_at // BLK) & (key_at <= query_at))
    own = jnp.exp(dot(k_ref[...], qs[...], 1, 1) * scale + jnp.where(need, less, MASKED))
    vdo = dot(v_ref[...], cs[...], 1, 1)
    gvo[...] = dot(own.astype(BF16), cs[...], 1, 0)
    first = jnp.sum(own * vdo, axis=0, keepdims=True)

    def relay(i):
        zz = z - 1 - i

        @pl.when(~is_far(zz, z))
        def _():
            z_copy(zz, zz).wait_recv()

            for yy in range(g):
                a, b = picked(zz, yy, lambda b: kz[zz, 0, b * BLK : (b + 1) * BLK, :],
                              lambda b: kz[zz, 1, b * BLK : (b + 1) * BLK, :])
                kvs[zz, yy, 0] = a
                kvs[zz, yy, 1] = b
            for k in far_first(g):
                y_copy(zz, lax.rem(y + k, g), y).start()
            kvt[zz * g + y] = kvs[zz, y]
    once = jnp.minimum(z, 1)
    each(0, once, relay)

    @pl.when(mine_far)
    def _():
        arrived(ff.at[pl.ds(0, g - 1)], fyr.at[0])
        far_z_copy(z).start()
    each(once, z, relay)

    loads[3].wait()
    width = x_ref.shape[1]
    w = width // tp
    eye = (iota((width, width), 0) == iota((width, width), 1)).astype(F32).astype(BF16)
    flipped = dot(eye, x_ref[...], 1, 1).astype(BF16)
    xs[...] = flipped.reshape(tp, w, tok)
    each_x1(0, lambda s: x1_copy(s, z).start())

    @pl.when(t == z)
    def _():
        xg[z] = xs[t]

    def send_back(c, zz):
        def one(k):
            yy = lax.rem(y + k, g)

            @pl.when((zz < z) | (yy < y))
            def _():
                back_copy(c, zz, yy, y).start()

        @pl.when(is_far_back(zz, z))
        def _():
            far_back_copy(c, zz).start()

        @pl.when(~is_far_back(zz, z))
        def _():
            for k in far_first(g):
                one(k)
            back_r[c, zz, y] = back_s[c, zz, y]

    def pass_one(i, delta):
        zz = z - i

        @pl.when(is_far(zz, z))
        def _():
            far_z_copy(zz).wait_recv()

        @pl.when((zz < z) & ~is_far(zz, z))
        def _():
            arrived(kvt.at[pl.ds(zz * g, g - 1)], yr_sem.at[zz])

        @pl.when(zz == z)
        def _():
            counted(y, g - 1, lambda i: arrived(kvt.at[pl.ds(z * g, i)], yr_sem.at[z]))
        kp = kvt[pl.ds(zz * g, g), 0].reshape(chunk, cols)
        vp = kvt[pl.ds(zz * g, g), 1].reshape(chunk, cols)
        line = jnp.concatenate(
            [jnp.broadcast_to(bias[zz, a : a + 1, :], (BLK, wide)) for a in range(g)], axis=0)
        weights = jnp.exp(dot(kp, qs[...], 1, 1) * scale + line)
        vd = dot(vp, cs[...], 1, 1)
        wts[zz] = weights
        vds[zz] = vd
        back_s[1, zz] = dot(weights.astype(BF16), cs[...], 1, 0).astype(BF16).reshape(g, BLK, cols)
        send_back(1, zz)
        return delta + jnp.sum(weights * vd, axis=0, keepdims=True)
    delta = lax.fori_loop(0, z + 1, pass_one, first)

    counted(tp - jnp.where(t == z, 1, 0), tp, lambda i: arrived(xg.at[pl.ds(0, i)], x1r.at[0]))
    for i in range(1, tp):
        x2_copy(lax.rem(t + i, tp), t).start()
    xr[t] = xg[...]

    dso = (own * (vdo - delta)).astype(BF16)
    dqa[...] = dot(dso, k_ref[...], 0, 0)

    def key_grads(zz):
        back_s[0, zz] = (dot(dss[zz], qs[...], 1, 0) * scale).astype(BF16).reshape(g, BLK, cols)
        send_back(0, zz)

    def pass_two(zz):
        kp = kvt[pl.ds(zz * g, g), 0].reshape(chunk, cols)
        ds = (wts[zz] * (vds[zz] - delta)).astype(BF16)
        dss[zz] = ds
        dqa[...] += dot(ds, kp, 0, 0)

        @pl.when(is_far_back(zz, z))
        def _():
            key_grads(zz)
    each(0, z + 1, pass_two)

    dq = jnp.where(low, dqa[:tok], dqa[tok:]) * scale
    dq = dq.astype(BF16)
    gq_ref[...] = dq
    dqr[z] = dq
    for i in far_first(r):
        dq_copy(lax.rem(z + i, r), z).start()

    def other_key_grads(zz):
        @pl.when(~is_far_back(zz, z))
        def _():
            key_grads(zz)
    each(0, z + 1, other_key_grads)
    gko[...] = dot(dso, qs[...], 1, 0) * scale

    def relay_back(c, low_z, high_z, with_own):
        own_sum = gko if c == 0 else gvo

        def own_add(i):
            yy = y + 1 + i
            got = back_r[c, z, yy].astype(F32)
            for b in range(bd):
                own_sum[b * BLK : (b + 1) * BLK, :] += got * mask(z, yy, b)

        def one(i):
            zz = i if c == 0 else z - 1 - i

            @pl.when(~is_far_back(zz, z))
            def _():
                arrived(back_r.at[c, zz, pl.ds(0, g - 1)], br_sem.at[c, zz])
                sums = [None] * bd
                for yy in range(g):
                    got = back_r[c, zz, yy].astype(F32)
                    for b in range(bd):
                        term = got * mask(zz, yy, b)
                        sums[b] = term if sums[b] is None else sums[b] + term
                for b in range(bd):
                    rel_s[c, zz, b * BLK : (b + 1) * BLK, :] = sums[b].astype(BF16)
                rel_copy(c, zz, z).start()
        each(low_z, high_z, one)
        if with_own:
            counted(g - 1 - y, g - 1, lambda i: arrived(back_r.at[c, z, pl.ds(0, i)], br_sem.at[c, z]))
            each(0, g - 1 - y, own_add)

    def far_forward(c):
        @pl.when(mine_far_back)
        def _():
            far_back_copy(c, 0).wait_recv()
            for i in far_first(g):
                far_ret_copy(c, lax.rem(y + i, g), y).start()

    def far_add(c):
        own_sum = gko if c == 0 else gvo

        @pl.when(mine_far_back)
        def _():
            arrived(fr.at[c, pl.ds(0, g - 1)], frr.at[c])
            fr[c, y] = fb[c, y]
            sums = [own_sum[b * BLK : (b + 1) * BLK, :] for b in range(bd)]
            for yy in range(g):
                got = fr[c, yy].astype(F32)
                for b in range(bd):
                    sums[b] = sums[b] + got * mask(r, yy, b)
            for b in range(bd):
                own_sum[b * BLK : (b + 1) * BLK, :] = sums[b]

    relay_back(1, 0, z, True)
    far_forward(1)
    far_forward(0)
    half = z // 2
    relay_back(0, 0, half, False)

    arrived(xr.at[pl.ds(0, tp - 1)], x2r.at[0])
    arrived(dqr.at[pl.ds(0, r - 1)], dqr_sem.at[0])
    total = None
    for zz in range(r):
        part = dot(xr[:, zz].reshape(width, tok), dqr[zz], 1, 0)
        total = part if total is None else total + part
    for yy in range(g):
        gs[yy] = total[yy * w : (yy + 1) * w].astype(BF16)

        @pl.when(yy == y)
        def _():
            gw_ref[...] = total[yy * w : (yy + 1) * w]
    for i in far_first(g):
        gw_copy(lax.rem(y + i, g), y).start()

    relay_back(0, half, z, True)
    far_add(1)
    far_add(0)

    def settle(c):
        own_sum = gko if c == 0 else gvo

        def one(i):
            zz = z + 1 + i

            @pl.when(~is_far_back(z, zz))
            def _():
                rel_copy(c, 0, zz).wait_recv()
                own_sum[...] += rel_r[c, zz].astype(F32)
        each(0, r - 1 - z, one)
        (gk_ref if c == 0 else gv_ref)[...] = own_sum[...].astype(BF16)
    settle(1)
    settle(0)

    arrived(gr.at[pl.ds(0, g - 1)], gr_sem.at[0])
    for i in range(1, g):
        gw_ref[...] += gr[lax.rem(y + i, g)].astype(F32)

    in_far = jnp.where(z == r - 1, 1, 0) + jnp.where(z == r - 2, 1, 0)
    counted(r - 1 - z - jnp.where(mine_far, 1, 0), r - 1, lambda i: left(kz.at[pl.ds(0, i)], zs_sem.at[0]))
    counted(g - 1 - y, g - 1, lambda i: left(kvs.at[z, pl.ds(0, i)], ys_sem.at[0]))

    @pl.when(mine_far)
    def _():
        far_z_copy(z).wait_send()
        left(fs.at[pl.ds(0, g - 1)], fys.at[0])

    @pl.when(mine_far_back)
    def _():
        left(fb.at[0, pl.ds(0, g - 1)], frs.at[0])
        left(fb.at[1, pl.ds(0, g - 1)], frs.at[1])

    for c in range(2):
        counted(z - in_far, r - 1, lambda i: left(rel_s.at[c, pl.ds(0, i)], rs_sem.at[c]))
        counted(y, g - 1, lambda i: left(back_s.at[c, z, pl.ds(0, i)], bs_sem.at[c]))

    def sent_row(zz):
        @pl.when(~is_far(zz, z))
        def _():
            left(kvs.at[zz, pl.ds(0, g - 1)], ys_sem.at[0])

        @pl.when(is_far_back(zz, z))
        def _():
            far_back_copy(0, zz).wait_send()
            far_back_copy(1, zz).wait_send()

        @pl.when(~is_far_back(zz, z))
        def _():
            left(back_s.at[0, zz, pl.ds(0, g - 1)], bs_sem.at[0])
            left(back_s.at[1, zz, pl.ds(0, g - 1)], bs_sem.at[1])
    each(0, z, sent_row)
    counted(tp - jnp.where(t == z, 1, 0), tp, lambda i: left(xs.at[pl.ds(0, i)], x1s.at[0]))
    left(xr.at[pl.ds(0, tp - 1)], x2s.at[0])
    left(dqr.at[pl.ds(0, r - 1)], dqs_sem.at[0])
    left(gs.at[pl.ds(0, g - 1)], gs_sem.at[0])


def write_out(*refs):
    sems = refs[8]
    copies = [pltpu.make_async_copy(refs[i], refs[4 + i], sems.at[i]) for i in range(4)]
    for copy in copies:
        copy.start()
    for copy in copies:
        copy.wait()


def body(g, r, tp, queries, keys, values, cotangent, log_sum, chosen, normed_input):
    tok, cols = queries.shape
    bd = tok // BLK
    wide = 2 * tok
    w = normed_input.shape[1] // tp
    vmem = pl.BlockSpec(memory_space=pltpu.VMEM)
    sem = pltpu.SemaphoreType.DMA
    hbm = pl.BlockSpec(memory_space=pltpu.HBM)
    picks = chosen.transpose(2, 0, 1)
    held = [pltpu.VMEM(a.shape, a.dtype) for a in (
        queries, jax.ShapeDtypeStruct((2, tok, cols), BF16), cotangent, log_sum, picks, normed_input)]
    made = pl.pallas_call(
        functools.partial(kernel, g, r, tp),
        out_shape=[
            jax.ShapeDtypeStruct((tok, cols), BF16),
            jax.ShapeDtypeStruct((tok, cols), BF16),
            jax.ShapeDtypeStruct((tok, cols), BF16),
            jax.ShapeDtypeStruct((w, cols), F32),
        ],
        in_specs=[hbm] * 7,
        out_specs=[vmem] * 4,
        scratch_shapes=held + [
            sem((7,)),
            pltpu.VMEM((wide, cols), BF16),
            pltpu.VMEM((wide, cols), BF16),
            pltpu.VMEM((r + 1, g, bd, cols), F32),
            pltpu.VMEM((r, g, wide), F32),
            pltpu.VMEM((r, 2, tok, cols), BF16),
            pltpu.VMEM((r, g, 2, BLK, cols), BF16),
            pltpu.VMEM((r * g, 2, BLK, cols), BF16),
            pltpu.VMEM((r, g * BLK, wide), F32),
            pltpu.VMEM((r, g * BLK, wide), F32),
            pltpu.VMEM((r, g * BLK, wide), BF16),
            pltpu.VMEM((2, r, g, BLK, cols), BF16),
            pltpu.VMEM((2, r, g, BLK, cols), BF16),
            pltpu.VMEM((2, r, tok, cols), BF16),
            pltpu.VMEM((2, r, tok, cols), BF16),
            pltpu.VMEM((tok, cols), F32),
            pltpu.VMEM((tok, cols), F32),
            pltpu.VMEM((wide, cols), F32),
            pltpu.VMEM((tp, w, tok), BF16),
            pltpu.VMEM((r, w, tok), BF16),
            pltpu.VMEM((tp, r, w, tok), BF16),
            pltpu.VMEM((r, tok, cols), BF16),
            pltpu.VMEM((g, w, cols), BF16),
            pltpu.VMEM((g, w, cols), BF16),
            pltpu.VMEM((g, 2, BLK, cols), BF16),
            pltpu.VMEM((g, 2, BLK, cols), BF16),
            pltpu.VMEM((2, g, BLK, cols), BF16),
            pltpu.VMEM((2, g, BLK, cols), BF16),
            sem((1,)), sem((r,)),
            sem((1,)), sem((r,)),
            sem((2,)), sem((2, r)),
            sem((2,)), sem((2, r)),
            sem((1,)), sem((1,)),
            sem((1,)), sem((1,)),
            sem((1,)), sem((1,)),
            sem((1,)), sem((1,)),
            sem((1,)), sem((1,)),
            sem((1,)), sem((2,)),
            sem((2, 2)), sem((2,)),
            sem((2,)), sem((2,)),
        ],
        compiler_params=pltpu.CompilerParams(
            has_side_effects=True, collective_id=0, vmem_limit_bytes=67043328),
    )(queries, keys, values, cotangent, log_sum, picks, normed_input)
    return pl.pallas_call(
        write_out,
        out_shape=[jax.ShapeDtypeStruct(a.shape, a.dtype) for a in made],
        in_specs=[vmem] * 4,
        out_specs=[hbm] * 4,
        scratch_shapes=[sem((4,))],
    )(*made)


def solution(mesh):
    n, tp = mesh.shape["kv"], mesh.shape["tp"]
    g = n // tp
    in_specs = (
        P("kv", "tp"), P("kv", "tp"), P("kv", "tp"), P("kv", "tp"),
        P("tp", "kv"), P("tp", None, None), P("kv", "tp"),
    )
    out_specs = (P("kv", "tp"),) * 4
    return jax.shard_map(
        functools.partial(body, g, n // g, tp), mesh=mesh, in_specs=in_specs, out_specs=out_specs, check_vma=False
    )
```
